32 devices in a mesh: sp: 8 (over z, x), dp: 4 (over y, core).
Axes of the slice: x: 2, y: 2, z: 4, core: 2. Of those that a mesh axis runs over, the one named last changes fastest.
Arguments:
- queries: bfloat16 [4, 1024, 2048], P('dp', 'sp'), may hold values from -6 to 6
- forget_pre: bfloat16 [4, 1024, 2048], P('dp', 'sp'), may hold values from -5.5 to 5.5
- values: bfloat16 [4, 1024, 2048], P('dp', 'sp'), may hold values from -6 to 6
- out_gate: bfloat16 [4, 1024, 2048], P('dp', 'sp'), may hold values from -6 to 6
- lower_bound: float32 [2048], P('sp'), may hold values from 0.9 to 1, as said below
- head_gain: float32 [128], replicated, may hold values from 0.1 to 1.9
- residual: bfloat16 [4, 1024, 4096], P('dp', 'sp'), may hold values from -6 to 6
- out_weight: bfloat16 [2048, 4096], P(None, 'dp'), may hold values from -0.125 to 0.125
- ffn_gain: float32 [4096], replicated, may hold values from 0.1 to 1.9
- routing: int32 [4, 1024, 4], P('dp', 'sp'), may hold values from 0 to 31, all different within a row; in each aligned block of 128 rows (0 to 127, 128 to 255, ..., all dimensions but the last counted through in order) at most 20 rows name the same one
- route_weight: float32 [4, 1024, 4], P('dp', 'sp'), may hold values from 0.1 to 1
- expert_gate: bfloat16 [32, 4096, 512], P(('sp', 'dp')), may hold values from -0.09375 to 0.09375
- expert_up: bfloat16 [32, 4096, 512], P(('sp', 'dp')), may hold values from -0.09375 to 0.09375
- expert_down: bfloat16 [32, 512, 4096], P(('sp', 'dp')), may hold values from -0.25 to 0.25
Outputs:
- layer_out: bfloat16 [4, 1024, 4096], P('dp', 'sp')
The draws below stay inside these ranges and needn't reach their ends.
Inputs may be any that keep to these rules, and one draw needn't show every extreme that they name: `routing`: within the rows of one device no expert is named more than 20 times, and in some devices one is named exactly 20 times; the 4 experts of a row differ. `lower_bound`: every entry is below 1.
All inputs are finite; a program needn't handle non-finite values.
Results may differ from the reference program's by a relative error of at most 0.0073.
Values may be sent and summed in bfloat16 or wider, within the bound.
A program may use at most 128 MiB of HBM per device.

```python
import math
import jax
import jax.numpy as jnp
import numpy as np
from jax import lax

D = 4096
HEADS = 16
HEAD_DIM = 128
A_WIDTH = 2048
FE = 512
EXPERTS = 32
TOP_K = 4
BLOCK = 128
TOK_DEV = 128
SEQLEN = 1024
CAP = 20
N_DP = 4


def draw_forget_pre(key, part):
    noise_key = jax.random.fold_in(key, 11)
    shift_key = jax.random.fold_in(key, 12)
    noise = jax.random.truncated_normal(noise_key, -4.0, 4.0, (N_DP, SEQLEN, A_WIDTH), jnp.float32)
    block_shift = jax.random.uniform(shift_key, (N_DP, SEQLEN // TOK_DEV, 1, 1), jnp.float32, -1.5, 1.5)
    noise = noise.reshape(N_DP, SEQLEN // TOK_DEV, TOK_DEV, A_WIDTH) + block_shift
    return noise.reshape(N_DP, SEQLEN, A_WIDTH).astype(jnp.bfloat16)


def draw_lower_bound(key, part):
    pick_key = jax.random.fold_in(key, 21)
    unit_key = jax.random.fold_in(key, 22)
    fast_heads = jax.random.randint(pick_key, (HEADS, 1), 0, 16) < 8
    unit_draw = jax.random.uniform(unit_key, (HEADS, HEAD_DIM), jnp.float32)
    slow_rate = 0.3 / SEQLEN * (20.0 / 3.0) ** unit_draw
    fast_rate = 1.0 / 50.0 * (50.0 / 15.0) ** unit_draw
    leak_rate = jnp.where(fast_heads, fast_rate, slow_rate)
    return (1.0 - leak_rate).reshape(A_WIDTH).astype(jnp.float32)


def shard_levels(own_key, shape, shards, low, high):
    def one(position, parts):
        steps = jax.random.uniform(jax.random.fold_in(jax.random.fold_in(own_key, 6), position), (parts,), jnp.float32, low / len(shards), high / len(shards))
        return jnp.repeat(jnp.exp(steps), shape[position] // parts).reshape((-1,) + (1,) * (len(shape) - position - 1))

    loudness = one(*shards[0])
    for cut in shards[1:]:
        loudness = loudness * one(*cut)
    return loudness


def shared_out(rng, own, number, rows, amount, top, most, skew):
    sequence = jax.random.permutation(rng, amount)
    crowded, usual = load_shares(amount, rows * top, most, skew, True), load_shares(amount, rows * top, most, skew, False)
    places = jnp.arange(amount)

    def named(tallies, rotation):
        used = int((tallies > 0).sum())
        fixed = max(1, used // 4)
        moved = fixed + (places - fixed + rotation * (used - fixed)) % max(1, amount - fixed)
        return jnp.zeros((amount,), jnp.int32).at[sequence[jnp.where(places < fixed, places, moved)]].set(jnp.asarray(tallies, jnp.int32))

    tallies = jnp.where(number % 4 == 0, named(crowded, number // 4), named(usual, number - number // 4 - 1))
    mixed = jax.random.permutation(jax.random.fold_in(own, 3), amount)
    source_of, sink = mixed[0:amount // 2 * 2:2], mixed[1:amount // 2 * 2:2]
    margin = jnp.minimum(tallies[source_of] - 1, most - tallies[sink]) // 2
    margin = jnp.where((source_of == sequence[0]) | (sink == sequence[0]) | (tallies[sink] == 0), 0, jnp.maximum(margin, 0))
    moved = jax.random.randint(jax.random.fold_in(own, 4), (amount // 2,), 0, 1 << 20) % (margin + 1)
    tallies = tallies.at[source_of].add(-moved).at[sink].add(moved)
    items = jnp.searchsorted(jnp.cumsum(tallies), jnp.arange(rows * top), side="right").astype(jnp.int32)
    table = items.reshape(top, rows).T
    table = table[jax.random.permutation(jax.random.fold_in(own, 1), rows)]
    rotation = jax.random.randint(jax.random.fold_in(own, 2), (rows, 1), 0, top)
    return jnp.take_along_axis(table, (jnp.arange(top)[None, :] + rotation) % top, axis=1)


def load_shares(number_of, total, limit, lean, full):
    portions = [(1 << 20) // math.isqrt(standing ** lean) + 1 for standing in range(1, number_of + 1)]
    largest = limit if full else min(limit, max(-(-total // number_of), total * portions[0] // sum(portions)))
    least = 1 if total - largest >= number_of - 1 else 0
    given, rest = [largest] + [least] * (number_of - 1), total - largest - least * (number_of - 1)
    while rest > 0:
        candidates = [i for i in range(1, number_of) if given[i] < largest] or [i for i in range(1, number_of) if given[i] < limit]
        mass, budget = sum([portions[i] for i in candidates]), rest
        for i in candidates:
            extra = min(limit - given[i], max(1, budget * portions[i] // mass), rest)
            given[i] = given[i] + extra
            rest = rest - extra
    return np.array(given)


def normal_values(stream_key, dims, scale, limit, pieces=(), kind=jnp.bfloat16):
    factor_of = shard_levels(stream_key, dims, pieces, -0.22, 0.18) if pieces else 1.0
    drawn = jax.random.normal(stream_key, dims, jnp.float32) * scale * factor_of
    return jnp.minimum(jnp.maximum(drawn, -limit), limit).astype(kind)


def setup_inputs(seed: int = 0) -> dict:
    keys = jax.random.split(jax.random.key(seed), 15)
    queries = normal_values(keys[0], (N_DP, SEQLEN, A_WIDTH), 1.0, 6.0, ((0, 4), (1, 8)))
    forget_pre = draw_forget_pre(jax.random.fold_in(keys[14], 71), 0)
    values = normal_values(keys[2], (N_DP, SEQLEN, A_WIDTH), 1.0, 6.0, ((0, 4), (1, 8)))
    out_gate = normal_values(keys[3], (N_DP, SEQLEN, A_WIDTH), 1.0, 6.0, ((0, 4), (1, 8)))
    lower_bound = draw_lower_bound(jax.random.fold_in(keys[14], 71), 0)
    head_gain = jnp.clip(1.0 + 0.18 * jax.random.normal(keys[5], (HEAD_DIM,), jnp.float32), 0.1, 1.9)
    residual = normal_values(keys[6], (N_DP, SEQLEN, D), 1.0, 6.0, ((0, 4), (1, 8)))
    out_weight = normal_values(keys[7], (A_WIDTH, D), A_WIDTH ** -0.5, 0.125, ((1, 4),))
    ffn_gain = jnp.clip(1.0 + 0.18 * jax.random.normal(keys[8], (D,), jnp.float32), 0.1, 1.9)
    routing_keys = jax.random.split(jax.random.fold_in(keys[9], 1), N_DP * SEQLEN // TOK_DEV)
    routing_turns = jax.random.permutation(jax.random.fold_in(keys[9], 3), N_DP * SEQLEN // TOK_DEV)
    routing = jax.vmap(lambda own, number: shared_out(jax.random.fold_in(keys[9], 2), own, number, TOK_DEV, EXPERTS, TOP_K, CAP, 2))(routing_keys, routing_turns).reshape((N_DP, SEQLEN, TOP_K))
    route_weight = jnp.clip(0.1 + 0.9 * jax.random.uniform(keys[10], (N_DP, SEQLEN, TOP_K), jnp.float32) ** shard_levels(keys[10], (N_DP, SEQLEN, TOP_K), ((0, 4), (1, 8)), -0.2, 0.2), 0.1, 1.0)
    expert_gate = normal_values(keys[11], (EXPERTS, D, FE), D ** -0.5, 0.09375, ((0, 32),))
    expert_up = normal_values(keys[12], (EXPERTS, D, FE), D ** -0.5, 0.09375, ((0, 32),))
    expert_down = normal_values(keys[13], (EXPERTS, FE, D), FE ** -0.5, 0.25, ((0, 32),))
    return dict(queries=queries, forget_pre=forget_pre, values=values, out_gate=out_gate, lower_bound=lower_bound, head_gain=head_gain, residual=residual, out_weight=out_weight, ffn_gain=ffn_gain, routing=routing, route_weight=route_weight, expert_gate=expert_gate, expert_up=expert_up, expert_down=expert_down)


PRECISE = lax.Precision.HIGHEST
NORM_EPS = 1e-06

def block_recurrence(query_f, log_keep, key_f, value_f):
    log_run = jnp.cumsum(log_keep, axis=1)
    log_last = log_run[:, -1]
    q_scaled = query_f * jnp.exp(log_run)
    k_scaled = key_f * jnp.exp(-log_run)
    k_carry = key_f * jnp.exp(log_last[:, None] - log_run)
    causal = jnp.tril(jnp.ones((BLOCK, BLOCK), bool))
    scores = jnp.einsum('nthk,nshk->nhts', q_scaled, k_scaled, precision=PRECISE)
    scores = jnp.where(causal, scores, 0.0)
    within = jnp.einsum('nhts,nshv->nthv', scores, value_f, precision=PRECISE)
    push_state = jnp.einsum('nshk,nshv->nhkv', k_carry, value_f, precision=PRECISE)
    keep_block = jnp.exp(log_last)

    def advance(state_now, block_item):
        keep_now, push_now = block_item
        return (keep_now[..., None] * state_now + push_now, state_now)
    start_state = jnp.zeros(push_state.shape[1:], jnp.float32)
    _, before = lax.scan(advance, start_state, (keep_block, push_state))
    carried = jnp.einsum('nthk,nhkv->nthv', q_scaled, before, precision=PRECISE)
    return within + carried

def reference(queries, forget_pre, values, out_gate, lower_bound, head_gain, residual, out_weight, ffn_gain, routing, route_weight, expert_gate, expert_up, expert_down):
    leak_rate = (1.0 - lower_bound) * jax.nn.sigmoid(-forget_pre.astype(jnp.float32))
    log_keep = jnp.log1p(-leak_rate)
    layout = (N_DP, SEQLEN // BLOCK, BLOCK, HEADS, HEAD_DIM)

    def one_sequence(seq_item):
        return block_recurrence(seq_item[0], seq_item[1], seq_item[2], seq_item[3])
    mix = lax.map(one_sequence, (queries.astype(jnp.float32).reshape(layout), log_keep.reshape(layout), leak_rate.reshape(layout), values.astype(jnp.float32).reshape(layout)))
    scale = lax.rsqrt(lax.optimization_barrier(jnp.mean(mix * mix, axis=-1, keepdims=True)) + NORM_EPS)
    normed = (mix * scale * head_gain).astype(jnp.bfloat16).reshape(N_DP * SEQLEN, A_WIDTH)
    gated_out = (normed.astype(jnp.float32) * jax.nn.silu(out_gate.reshape(N_DP * SEQLEN, A_WIDTH).astype(jnp.float32))).astype(jnp.bfloat16)
    projected = jnp.dot(gated_out, out_weight, preferred_element_type=jnp.float32).astype(jnp.bfloat16)
    hidden = (residual.reshape(N_DP * SEQLEN, D).astype(jnp.float32) + projected.astype(jnp.float32)).astype(jnp.bfloat16)
    hidden_f = hidden.astype(jnp.float32)
    moe_in = (hidden_f * lax.rsqrt(lax.optimization_barrier(jnp.mean(hidden_f * hidden_f, axis=-1, keepdims=True)) + NORM_EPS) * ffn_gain).astype(jnp.bfloat16)
    all_rows = N_DP * SEQLEN
    blocks = all_rows // TOK_DEV
    per_expert = blocks * CAP
    chosen = routing.reshape(blocks, TOK_DEV * TOP_K).astype(jnp.int32)
    matches = (chosen[:, :, None] == jnp.arange(EXPERTS, dtype=jnp.int32)[None, None, :]).astype(jnp.int32)
    rank_in = lax.optimization_barrier(jnp.sum((jnp.cumsum(matches, axis=1) - 1) * matches, axis=2)).astype(jnp.int32)
    target = chosen * per_expert + jnp.arange(blocks, dtype=jnp.int32)[:, None] * CAP + rank_in
    target = target.reshape(-1).astype(jnp.int32)
    owners = jnp.arange(all_rows * TOP_K, dtype=jnp.int32) // TOP_K
    slot_owner = jnp.full((EXPERTS * per_expert,), all_rows, jnp.int32).at[target].set(owners)
    slot_weight = jnp.zeros((EXPERTS * per_expert,), jnp.float32).at[target].set(route_weight.reshape(-1))
    padded = jnp.concatenate([moe_in, jnp.zeros((1, D), jnp.bfloat16)], axis=0)

    def add_expert(weighted, expert_item):
        owner_rows, weight_rows, w_gate, w_up, w_down = expert_item
        slot_rows = padded[owner_rows]
        gate_part = jnp.dot(slot_rows, w_gate, preferred_element_type=jnp.float32)
        up_part = jnp.dot(slot_rows, w_up, preferred_element_type=jnp.float32)
        act = (jax.nn.silu(gate_part) * up_part).astype(jnp.bfloat16)
        expert_out = jnp.dot(act, w_down, preferred_element_type=jnp.float32).astype(jnp.bfloat16)
        return (weighted.at[owner_rows].add(expert_out.astype(jnp.float32) * weight_rows[:, None]), None)
    weighted, _ = lax.scan(add_expert, jnp.zeros((all_rows + 1, D), jnp.float32), (slot_owner.reshape(EXPERTS, per_expert), slot_weight.reshape(EXPERTS, per_expert), expert_gate, expert_up, expert_down))
    layer_out = (hidden_f + weighted[:all_rows]).astype(jnp.bfloat16)
    return layer_out.reshape(N_DP, SEQLEN, D)
```

```python
import functools

import jax
import jax.numpy as jnp
from jax import lax
from jax.experimental import pallas as pl
from jax.experimental.pallas import tpu as pltpu
from jax.sharding import PartitionSpec as P

MESH = pl.DeviceIdType.MESH
VMEM_WHOLE = pl.BlockSpec(memory_space=pltpu.VMEM)

BLOCK = 128
CHUNK = 512


PRECISE = lax.Precision.HIGHEST
NORM_EPS = 1e-06


def forget_terms(forget_pre, lower_bound):
    leak_rate = (1.0 - lower_bound) * jax.nn.sigmoid(-forget_pre.astype(jnp.float32))
    return (jnp.log1p(-leak_rate), leak_rate)


def link_states(earlier, later):
    return (earlier[0] * later[0], later[0][..., None] * earlier[1] + later[1])


def recurrence(query_f, log_keep, key_f, value_f):
    log_run = jnp.cumsum(log_keep, axis=1)
    log_last = log_run[:, -1]
    q_scaled = query_f * jnp.exp(log_run)
    k_scaled = key_f * jnp.exp(-log_run)
    k_carry = key_f * jnp.exp(log_last[:, None] - log_run)
    causal = jnp.tril(jnp.ones((BLOCK, BLOCK), bool))
    scores = jnp.einsum("nthk,nshk->nhts", q_scaled, k_scaled, precision=PRECISE)
    scores = jnp.where(causal, scores, 0.0)
    within = jnp.einsum("nhts,nshv->nthv", scores, value_f, precision=PRECISE)
    push_state = jnp.einsum("nshk,nshv->nhkv", k_carry, value_f, precision=PRECISE)
    keep_block = jnp.exp(log_last)
    keep_run, state_run = lax.associative_scan(link_states, (keep_block, push_state), axis=0)
    before = jnp.concatenate([jnp.zeros_like(state_run[:1]), state_run[:-1]], axis=0)
    keep_before = jnp.concatenate([jnp.ones_like(keep_run[:1]), keep_run[:-1]], axis=0)
    carried = jnp.einsum("nthk,nhkv->nthv", q_scaled, before, precision=PRECISE)
    return (within + carried, q_scaled * keep_before[:, None], keep_run[-1], state_run[-1])


def head_norm(mixer_out, head_gain):
    scale = lax.rsqrt(jnp.mean(mixer_out * mixer_out, axis=-1, keepdims=True) + NORM_EPS)
    return (mixer_out * scale * head_gain).astype(jnp.bfloat16)


def wait_bytes(ref, sem):
    pltpu.make_async_copy(ref, ref, sem).wait()


def place(nz, nx, ndp):
    sp, dp = lax.axis_index("sp"), lax.axis_index("dp")
    z = lax.div(sp, nx)
    me = lax.rem(sp, nx) * ndp + dp
    above, below = {"sp": sp + nx, "dp": dp}, {"sp": sp - nx, "dp": dp}

    def member(p):
        return {"sp": z * nx + lax.div(p, ndp), "dp": lax.rem(p, ndp)}

    return z, me, above, below, member


def greet(nz, peers, z, me, above, below, member):
    barrier = pltpu.get_barrier_semaphore()

    @pl.when(z > 0)
    def _():
        pl.semaphore_signal(barrier, inc=1, device_id=below, device_id_type=MESH)

    @pl.when(z < nz - 1)
    def _():
        pl.semaphore_signal(barrier, inc=1, device_id=above, device_id_type=MESH)

    def one(k, carry):
        pl.semaphore_signal(
            barrier, inc=1, device_id=member(lax.rem(me + k, peers)), device_id_type=MESH
        )
        return carry

    lax.fori_loop(1, peers, one, 0)
    count = peers - 1 + jnp.where(z > 0, 1, 0) + jnp.where(z < nz - 1, 1, 0)
    pl.semaphore_wait(barrier, count)


def dispatch_kernel(
    nz, nx, ndp, width, x_ref, pick_ref, out_ref, gath, slots, up_send, dn_send, line_recv, pl_send, pl_recv
):
    peers = nx * ndp
    z, me, above, below, member = place(nz, nx, ndp)
    tok, model = x_ref.shape
    chunks = model // width
    per = out_ref.shape[0] // peers
    greet(nz, peers, z, me, above, below, member)

    def block(b):
        return pl.ds(pl.multiple_of(b * tok, tok), tok)

    def share(p):
        return pl.ds(pl.multiple_of(p * per, per), per)

    def pass_on(src, b, c, cols, sem, device):
        pltpu.make_async_remote_copy(
            src_ref=src,
            dst_ref=gath.at[block(b), cols],
            send_sem=sem,
            recv_sem=line_recv.at[b, c],
            device_id=device,
            device_id_type=MESH,
        ).start()

    gath[block(z), :] = x_ref[...]

    def tick(t, carry):
        for s in range(nz):
            c = t - s
            cols = pl.ds(pl.multiple_of(c * width, width), width)
            valid = (c >= 0) & (c < chunks)
            if s == 0:

                @pl.when(valid & (z < nz - 1))
                def _():
                    pass_on(x_ref.at[:, cols], z, c, cols, up_send.at[0], above)

                @pl.when(valid & (z > 0))
                def _():
                    pass_on(x_ref.at[:, cols], z, c, cols, dn_send.at[0], below)

                continue

            @pl.when(valid & (z - s >= 0))
            def _():
                b = z - s
                here = gath.at[block(b), cols]
                wait_bytes(here, line_recv.at[b, c])

                @pl.when(z < nz - 1)
                def _():
                    pass_on(here, b, c, cols, up_send.at[s], above)

            @pl.when(valid & (z + s < nz))
            def _():
                b = z + s
                here = gath.at[block(b), cols]
                wait_bytes(here, line_recv.at[b, c])

                @pl.when(z > 0)
                def _():
                    pass_on(here, b, c, cols, dn_send.at[s], below)

        c = t - (nz - 1)

        @pl.when(c >= 0)
        def _():
            cols = pl.ds(pl.multiple_of(c * width, width), width)
            slots[:, cols] = jnp.dot(
                pick_ref[...], gath[:, cols], preferred_element_type=jnp.float32
            ).astype(jnp.bfloat16)
            out_ref[share(me), cols] = slots[share(me), cols]

            def send(k, inner):
                p = lax.rem(me + k, peers)
                pltpu.make_async_remote_copy(
                    src_ref=slots.at[share(p), cols],
                    dst_ref=out_ref.at[share(me), cols],
                    send_sem=pl_send.at[k],
                    recv_sem=pl_recv.at[k],
                    device_id=member(p),
                    device_id_type=MESH,
                ).start()
                return inner

            lax.fori_loop(1, peers, send, 0)

        return carry

    lax.fori_loop(0, chunks + nz - 1, tick, 0)

    for s in range(nz - 1):

        @pl.when((z - s >= 0) & (z < nz - 1))
        def _():
            wait_bytes(x_ref, up_send.at[s])

        @pl.when((z + s < nz) & (z > 0))
        def _():
            wait_bytes(x_ref, dn_send.at[s])

    def finish(k, carry):
        wait_bytes(slots.at[share(lax.rem(me + k, peers)), :], pl_send.at[k])
        wait_bytes(out_ref.at[share(lax.rem(me + peers - k, peers)), :], pl_recv.at[k])
        return carry

    lax.fori_loop(1, peers, finish, 0)


def return_kernel(
    nz,
    nx,
    ndp,
    width,
    r_ref,
    high_ref,
    low_ref,
    h_ref,
    out_ref,
    ret,
    part,
    up_out,
    up_in,
    dn_out,
    dn_in,
    pl_send,
    pl_recv,
    up_send,
    dn_send,
    up_recv,
    dn_recv,
):
    peers = nx * ndp
    z, me, above, below, member = place(nz, nx, ndp)
    tok, model = h_ref.shape
    chunks = model // width
    per = r_ref.shape[0] // peers
    greet(nz, peers, z, me, above, below, member)

    def block(b):
        return pl.ds(pl.multiple_of(b * tok, tok), tok)

    def share(p):
        return pl.ds(pl.multiple_of(p * per, per), per)

    def columns(c):
        return pl.ds(pl.multiple_of(c * width, width), width)

    def send_chunk(c, carry):
        def send(k, inner):
            p = lax.rem(me + k, peers)
            pltpu.make_async_remote_copy(
                src_ref=r_ref.at[share(p), columns(c)],
                dst_ref=ret.at[share(me), columns(c)],
                send_sem=pl_send.at[k],
                recv_sem=pl_recv.at[k, c],
                device_id=member(p),
                device_id_type=MESH,
            ).start()
            return inner

        return lax.fori_loop(1, peers, send, carry)

    lax.fori_loop(0, chunks, send_chunk, 0)
    ret[share(me), :] = r_ref[share(me), :]

    def line(c, first, sends, takes, inbox, outbox, send_sem, recv_sem, device):
        cols = columns(c)
        for d in range(nz):
            rows = pl.ds(d * tok, tok)

            @pl.when(jnp.logical_not(first) & takes(d))
            def _():
                wait_bytes(inbox.at[rows, cols], recv_sem.at[d, c])

            @pl.when(sends(d))
            def _():
                @pl.when(first)
                def _():
                    outbox[rows, cols] = part[rows, cols].astype(jnp.bfloat16)

                @pl.when(jnp.logical_not(first))
                def _():
                    outbox[rows, cols] = (
                        part[rows, cols] + inbox[rows, cols].astype(jnp.float32)
                    ).astype(jnp.bfloat16)

                pltpu.make_async_remote_copy(
                    src_ref=outbox.at[rows, cols],
                    dst_ref=inbox.at[rows, cols],
                    send_sem=send_sem.at[d],
                    recv_sem=recv_sem.at[d, c],
                    device_id=device,
                    device_id_type=MESH,
                ).start()

    def tick(t, carry):
        @pl.when(t < chunks)
        def _():
            cols = columns(t)

            def arrive(k, inner):
                p = lax.rem(me + peers - k, peers)
                wait_bytes(ret.at[share(p), cols], pl_recv.at[k, t])
                return inner

            lax.fori_loop(1, peers, arrive, 0)
            rows = ret[:, cols]
            part[:, cols] = jnp.dot(
                high_ref[...], rows, preferred_element_type=jnp.float32
            ) + jnp.dot(low_ref[...], rows, preferred_element_type=jnp.float32)

        cu = t - z

        @pl.when((cu >= 0) & (cu < chunks))
        def _():
            line(
                cu, z == 0, lambda d: d > z, lambda d: d >= z, up_in, up_out, up_send, up_recv, above
            )

        cd = t - (nz - 1 - z)

        @pl.when((cd >= 0) & (cd < chunks))
        def _():
            line(
                cd, z == nz - 1, lambda d: d < z, lambda d: d <= z, dn_in, dn_out, dn_send, dn_recv, below
            )

        return carry

    lax.fori_loop(0, chunks + nz - 1, tick, 0)

    own = block(z)

    @pl.when(z > 0)
    def _():
        part[own, :] = part[own, :] + up_in[own, :].astype(jnp.float32)

    @pl.when(z < nz - 1)
    def _():
        part[own, :] = part[own, :] + dn_in[own, :].astype(jnp.float32)

    out_ref[...] = (h_ref[...].astype(jnp.float32) + part[own, :]).astype(jnp.bfloat16)

    for d in range(nz):

        @pl.when(d > z)
        def _():
            wait_bytes(up_out.at[pl.ds(d * tok, tok), :], up_send.at[d])

        @pl.when(d < z)
        def _():
            wait_bytes(dn_out.at[pl.ds(d * tok, tok), :], dn_send.at[d])

    def finish(k, carry):
        wait_bytes(r_ref.at[share(lax.rem(me + k, peers)), :], pl_send.at[k])
        return carry

    lax.fori_loop(1, peers, finish, 0)


def routing_tables(routing, route_weight, nz, nx, ndp, cap, per):
    tok, top = routing.shape
    peers = nx * ndp
    packed = jnp.concatenate([routing.astype(jnp.float32), route_weight], axis=1)
    packed = lax.all_gather(packed, "sp", axis=0)
    sp = lax.axis_index("sp")
    z, x = sp // nx, sp % nx
    packed = lax.dynamic_index_in_dim(packed.reshape(nz, nx, tok, 2 * top), x, 1, keepdims=False)
    chosen = packed[..., :top].astype(jnp.int32)
    experts = z * peers + jnp.arange(peers, dtype=jnp.int32)
    same = chosen[:, :, :, None] == experts
    named = jnp.any(same, axis=2)
    weight = jnp.sum(jnp.where(same, packed[..., top:, None], 0.0), axis=2)
    earlier = jnp.tril(jnp.ones((tok, tok), jnp.bfloat16), -1)
    rank = jnp.einsum(
        "ts,bsp->btp", earlier, named.astype(jnp.bfloat16), preferred_element_type=jnp.float32
    ).astype(jnp.int32)
    slot = jnp.arange(nz, dtype=jnp.int32)[:, None, None] * cap + rank
    slot = jnp.where(named, slot, per)
    slot_ids = jnp.arange(per, dtype=jnp.int32)
    pick = slot.transpose(2, 0, 1)[:, None, :, :] == slot_ids[None, :, None, None]
    pick = pick.astype(jnp.bfloat16).reshape(peers * per, nz * tok)
    mixed = jnp.where(slot[..., None] == slot_ids, weight[..., None], 0.0)
    mixed = mixed.reshape(nz * tok, peers * per)
    high = lax.reduce_precision(mixed, 8, 7)
    return pick, high.astype(jnp.bfloat16), (mixed - high).astype(jnp.bfloat16)


def dispatch(moe_in, pick, nz, nx, ndp, width):
    tok, model = moe_in.shape
    peers = nx * ndp
    total = pick.shape[0]
    chunks = model // width
    bf16 = jnp.bfloat16
    return pl.pallas_call(
        functools.partial(dispatch_kernel, nz, nx, ndp, width),
        out_shape=jax.ShapeDtypeStruct((total, model), bf16),
        in_specs=[VMEM_WHOLE] * 2,
        out_specs=VMEM_WHOLE,
        scratch_shapes=[
            pltpu.VMEM((nz * tok, model), bf16),
            pltpu.VMEM((total, model), bf16),
            pltpu.SemaphoreType.DMA((nz,)),
            pltpu.SemaphoreType.DMA((nz,)),
            pltpu.SemaphoreType.DMA((nz, chunks)),
            pltpu.SemaphoreType.DMA((peers,)),
            pltpu.SemaphoreType.DMA((peers,)),
        ],
        compiler_params=pltpu.CompilerParams(
            collective_id=1, has_side_effects=True, vmem_limit_bytes=60 * 1024 * 1024
        ),
    )(moe_in, pick)


def combine(results, high, low, hidden, nz, nx, ndp, width):
    tok, model = hidden.shape
    peers = nx * ndp
    total = results.shape[0]
    chunks = model // width
    bf16 = jnp.bfloat16
    return pl.pallas_call(
        functools.partial(return_kernel, nz, nx, ndp, width),
        out_shape=jax.ShapeDtypeStruct((tok, model), bf16),
        in_specs=[VMEM_WHOLE] * 4,
        out_specs=VMEM_WHOLE,
        scratch_shapes=[
            pltpu.VMEM((total, model), bf16),
            pltpu.VMEM((nz * tok, model), jnp.float32),
            pltpu.VMEM((nz * tok, model), bf16),
            pltpu.VMEM((nz * tok, model), bf16),
            pltpu.VMEM((nz * tok, model), bf16),
            pltpu.VMEM((nz * tok, model), bf16),
            pltpu.SemaphoreType.DMA((peers,)),
            pltpu.SemaphoreType.DMA((peers, chunks)),
            pltpu.SemaphoreType.DMA((nz,)),
            pltpu.SemaphoreType.DMA((nz,)),
            pltpu.SemaphoreType.DMA((nz, chunks)),
            pltpu.SemaphoreType.DMA((nz, chunks)),
        ],
        compiler_params=pltpu.CompilerParams(
            collective_id=2, has_side_effects=True, vmem_limit_bytes=60 * 1024 * 1024
        ),
    )(results, high, low, hidden)


def expert_mlp(slot_rows, w_gate, w_up, w_down):
    gate_part = jnp.dot(slot_rows, w_gate, preferred_element_type=jnp.float32)
    up_part = jnp.dot(slot_rows, w_up, preferred_element_type=jnp.float32)
    act = (jax.nn.silu(gate_part) * up_part).astype(jnp.bfloat16)
    return jnp.dot(act, w_down, preferred_element_type=jnp.float32).astype(jnp.bfloat16)


def local(
    queries,
    forget_pre,
    values,
    out_gate,
    lower_bound,
    head_gain,
    residual,
    out_weight,
    ffn_gain,
    routing,
    route_weight,
    expert_gate,
    expert_up,
    expert_down,
):
    tok_rows = queries.shape[1]
    head_size = head_gain.shape[0]
    model_width = residual.shape[2]
    arrived = (
        lax.all_to_all(queries, "sp", split_axis=2, concat_axis=1, tiled=True),
        lax.all_to_all(forget_pre, "sp", split_axis=2, concat_axis=1, tiled=True),
        lax.all_to_all(values, "sp", split_axis=2, concat_axis=1, tiled=True),
    )
    seq_rows = arrived[0].shape[1]
    own_heads = arrived[0].shape[2] // head_size
    log_keep, leak_rate = forget_terms(arrived[1], lower_bound)
    layout = (seq_rows // BLOCK, BLOCK, own_heads, head_size)
    mixer_out, _, _, _ = recurrence(
        arrived[0].astype(jnp.float32).reshape(layout),
        log_keep.reshape(layout),
        leak_rate.reshape(layout),
        arrived[2].astype(jnp.float32).reshape(layout),
    )
    normed = head_norm(mixer_out, head_gain).reshape(1, seq_rows, own_heads * head_size)
    normed = lax.all_to_all(normed, "sp", split_axis=1, concat_axis=2, tiled=True)
    gated_out = (normed.astype(jnp.float32) * jax.nn.silu(out_gate.astype(jnp.float32))).astype(
        jnp.bfloat16
    )
    columns = jnp.einsum(
        "ntc,cd->ntd",
        lax.all_gather(gated_out, "dp", axis=0, tiled=True),
        out_weight,
        preferred_element_type=jnp.float32,
    ).astype(jnp.bfloat16)
    projected = lax.all_to_all(columns, "dp", split_axis=0, concat_axis=2, tiled=True)
    hidden = (residual.astype(jnp.float32) + projected.astype(jnp.float32)).astype(jnp.bfloat16)
    hidden_f = hidden.astype(jnp.float32).reshape(tok_rows, model_width)
    moe_in = (
        hidden_f
        * lax.rsqrt(jnp.mean(hidden_f * hidden_f, axis=-1, keepdims=True) + NORM_EPS)
        * ffn_gain
    ).astype(jnp.bfloat16)
    top_count = routing.shape[2]
    span_sp = lax.axis_size("sp")
    span_dp = lax.axis_size("dp")
    experts = expert_gate.shape[0] * span_sp * span_dp
    cap = max(2, 5 * tok_rows * top_count // (4 * experts))
    nx = span_dp // 2
    nz = span_sp // nx
    per = -(-nz * cap // 16) * 16
    width = min(CHUNK, model_width)
    hidden = hidden.reshape(tok_rows, model_width)
    pick, high, low = routing_tables(
        routing.reshape(tok_rows, top_count),
        route_weight.reshape(tok_rows, top_count),
        nz,
        nx,
        span_dp,
        cap,
        per,
    )
    slot_rows = dispatch(moe_in, pick, nz, nx, span_dp, width)
    results = expert_mlp(slot_rows, expert_gate[0], expert_up[0], expert_down[0])
    layer_out = combine(results, high, low, hidden, nz, nx, span_dp, width)
    return layer_out.reshape(1, tok_rows, model_width)


def solution(mesh):
    in_specs = (
        P("dp", "sp", None),
        P("dp", "sp", None),
        P("dp", "sp", None),
        P("dp", "sp", None),
        P("sp"),
        P(),
        P("dp", "sp", None),
        P(None, "dp"),
        P(),
        P("dp", "sp", None),
        P("dp", "sp", None),
        P(("sp", "dp"), None, None),
        P(("sp", "dp"), None, None),
        P(("sp", "dp"), None, None),
    )
    out_specs = P("dp", "sp", None)
    return jax.shard_map(local, mesh=mesh, in_specs=in_specs, out_specs=out_specs, check_vma=False)
```

```python
import functools

import jax
import jax.numpy as jnp
from jax import lax
from jax.experimental import pallas as pl
from jax.experimental.pallas import tpu as pltpu
from jax.sharding import PartitionSpec as P

MESH = pl.DeviceIdType.MESH
VMEM_WHOLE = pl.BlockSpec(memory_space=pltpu.VMEM)

CHUNK = 512
GATED_PARTS = 4


NORM_EPS = 1e-06


def wait_bytes(ref, sem):
    pltpu.make_async_copy(ref, ref, sem).wait()


def place(nz, nx, ndp):
    sp, dp = lax.axis_index("sp"), lax.axis_index("dp")
    z = lax.div(sp, nx)
    me = lax.rem(sp, nx) * ndp + dp
    above, below = {"sp": sp + nx, "dp": dp}, {"sp": sp - nx, "dp": dp}

    def member(p):
        return {"sp": z * nx + lax.div(p, ndp), "dp": lax.rem(p, ndp)}

    return z, me, above, below, member


def greet(nz, peers, z, me, above, below, member):
    barrier = pltpu.get_barrier_semaphore()

    @pl.when(z > 0)
    def _():
        pl.semaphore_signal(barrier, inc=1, device_id=below, device_id_type=MESH)

    @pl.when(z < nz - 1)
    def _():
        pl.semaphore_signal(barrier, inc=1, device_id=above, device_id_type=MESH)

    def one(k, carry):
        pl.semaphore_signal(
            barrier, inc=1, device_id=member(lax.rem(me + k, peers)), device_id_type=MESH
        )
        return carry

    lax.fori_loop(1, peers, one, 0)
    count = peers - 1 + jnp.where(z > 0, 1, 0) + jnp.where(z < nz - 1, 1, 0)
    pl.semaphore_wait(barrier, count)


def dispatch_kernel(
    nz,
    nx,
    ndp,
    width,
    x_ref,
    pick_ref,
    gate_ref,
    lift_ref,
    act_ref,
    gath,
    slots,
    got,
    gate_sum,
    lift_sum,
    up_send,
    dn_send,
    line_recv,
    pl_send,
    pl_recv,
):
    peers = nx * ndp
    z, me, above, below, member = place(nz, nx, ndp)
    tok, model = x_ref.shape
    chunks = model // width
    per = act_ref.shape[0] // peers
    greet(nz, peers, z, me, above, below, member)

    def block(b):
        return pl.ds(pl.multiple_of(b * tok, tok), tok)

    def share(p):
        return pl.ds(pl.multiple_of(p * per, per), per)

    def pass_on(src, b, c, cols, sem, device):
        pltpu.make_async_remote_copy(
            src_ref=src,
            dst_ref=gath.at[block(b), cols],
            send_sem=sem,
            recv_sem=line_recv.at[b, c],
            device_id=device,
            device_id_type=MESH,
        ).start()

    gath[block(z), :] = x_ref[...]
    gate_sum[...] = jnp.zeros_like(gate_sum)
    lift_sum[...] = jnp.zeros_like(lift_sum)

    def tick(t, carry):
        for s in range(nz):
            c = t - s
            cols = pl.ds(pl.multiple_of(c * width, width), width)
            valid = (c >= 0) & (c < chunks)
            if s == 0:

                @pl.when(valid & (z < nz - 1))
                def _():
                    pass_on(x_ref.at[:, cols], z, c, cols, up_send.at[0], above)

                @pl.when(valid & (z > 0))
                def _():
                    pass_on(x_ref.at[:, cols], z, c, cols, dn_send.at[0], below)

                continue

            @pl.when(valid & (z - s >= 0))
            def _():
                b = z - s
                here = gath.at[block(b), cols]
                wait_bytes(here, line_recv.at[b, c])

                @pl.when(z < nz - 1)
                def _():
                    pass_on(here, b, c, cols, up_send.at[s], above)

            @pl.when(valid & (z + s < nz))
            def _():
                b = z + s
                here = gath.at[block(b), cols]
                wait_bytes(here, line_recv.at[b, c])

                @pl.when(z > 0)
                def _():
                    pass_on(here, b, c, cols, dn_send.at[s], below)

        c = t - (nz - 1)

        @pl.when((c >= 0) & (c < chunks))
        def _():
            cols = pl.ds(pl.multiple_of(c * width, width), width)
            slots[:, cols] = jnp.dot(
                pick_ref[...], gath[:, cols], preferred_element_type=jnp.float32
            ).astype(jnp.bfloat16)
            got[share(me), cols] = slots[share(me), cols]

            def send(k, inner):
                p = lax.rem(me + k, peers)
                pltpu.make_async_remote_copy(
                    src_ref=slots.at[share(p), cols],
                    dst_ref=got.at[share(me), cols],
                    send_sem=pl_send.at[k],
                    recv_sem=pl_recv.at[k, c],
                    device_id=member(p),
                    device_id_type=MESH,
                ).start()
                return inner

            lax.fori_loop(1, peers, send, 0)

        late = t - nz

        @pl.when(late >= 0)
        def _():
            cols = pl.ds(pl.multiple_of(late * width, width), width)

            def arrive(k, inner):
                p = lax.rem(me + peers - k, peers)
                wait_bytes(got.at[share(p), cols], pl_recv.at[k, late])
                return inner

            lax.fori_loop(1, peers, arrive, 0)
            rows = got[:, cols]
            gate_sum[...] += jnp.dot(rows, gate_ref[cols, :], preferred_element_type=jnp.float32)
            lift_sum[...] += jnp.dot(rows, lift_ref[cols, :], preferred_element_type=jnp.float32)

        return carry

    lax.fori_loop(0, chunks + nz, tick, 0)
    gate = gate_sum[...]
    act_ref[...] = (gate / (1.0 + jnp.exp(-gate)) * lift_sum[...]).astype(jnp.bfloat16)

    for s in range(nz - 1):

        @pl.when((z - s >= 0) & (z < nz - 1))
        def _():
            wait_bytes(x_ref, up_send.at[s])

        @pl.when((z + s < nz) & (z > 0))
        def _():
            wait_bytes(x_ref, dn_send.at[s])

    def finish(k, carry):
        wait_bytes(slots.at[share(lax.rem(me + k, peers)), :], pl_send.at[k])
        return carry

    lax.fori_loop(1, peers, finish, 0)


def return_kernel(
    nz,
    nx,
    ndp,
    width,
    act_ref,
    down_ref,
    high_ref,
    low_ref,
    h_ref,
    out_ref,
    r_ref,
    ret,
    part,
    up_out,
    up_in,
    dn_out,
    dn_in,
    pl_send,
    pl_recv,
    up_send,
    dn_send,
    up_recv,
    dn_recv,
):
    peers = nx * ndp
    z, me, above, below, member = place(nz, nx, ndp)
    tok, model = h_ref.shape
    chunks = model // width
    per = r_ref.shape[0] // peers
    greet(nz, peers, z, me, above, below, member)

    def block(b):
        return pl.ds(pl.multiple_of(b * tok, tok), tok)

    def share(p):
        return pl.ds(pl.multiple_of(p * per, per), per)

    def columns(c):
        return pl.ds(pl.multiple_of(c * width, width), width)

    def send_chunk(c, carry):
        r_ref[:, columns(c)] = jnp.dot(
            act_ref[...], down_ref[:, columns(c)], preferred_element_type=jnp.float32
        ).astype(jnp.bfloat16)

        def send(k, inner):
            p = lax.rem(me + k, peers)
            pltpu.make_async_remote_copy(
                src_ref=r_ref.at[share(p), columns(c)],
                dst_ref=ret.at[share(me), columns(c)],
                send_sem=pl_send.at[k],
                recv_sem=pl_recv.at[k, c],
                device_id=member(p),
                device_id_type=MESH,
            ).start()
            return inner

        return lax.fori_loop(1, peers, send, carry)

    lax.fori_loop(0, chunks, send_chunk, 0)
    ret[share(me), :] = r_ref[share(me), :]

    def line(c, first, sends, takes, inbox, outbox, send_sem, recv_sem, device):
        cols = columns(c)
        for d in range(nz):
            rows = pl.ds(d * tok, tok)

            @pl.when(jnp.logical_not(first) & takes(d))
            def _():
                wait_bytes(inbox.at[rows, cols], recv_sem.at[d, c])

            @pl.when(sends(d))
            def _():
                @pl.when(first)
                def _():
                    outbox[rows, cols] = part[rows, cols].astype(jnp.bfloat16)

                @pl.when(jnp.logical_not(first))
                def _():
                    outbox[rows, cols] = (
                        part[rows, cols] + inbox[rows, cols].astype(jnp.float32)
                    ).astype(jnp.bfloat16)

                pltpu.make_async_remote_copy(
                    src_ref=outbox.at[rows, cols],
                    dst_ref=inbox.at[rows, cols],
                    send_sem=send_sem.at[d],
                    recv_sem=recv_sem.at[d, c],
                    device_id=device,
                    device_id_type=MESH,
                ).start()

    def tick(t, carry):
        @pl.when(t < chunks)
        def _():
            cols = columns(t)

            def arrive(k, inner):
                p = lax.rem(me + peers - k, peers)
                wait_bytes(ret.at[share(p), cols], pl_recv.at[k, t])
                return inner

            lax.fori_loop(1, peers, arrive, 0)
            rows = ret[:, cols]
            part[:, cols] = jnp.dot(
                high_ref[...], rows, preferred_element_type=jnp.float32
            ) + jnp.dot(low_ref[...], rows, preferred_element_type=jnp.float32)

        cu = t - z

        @pl.when((cu >= 0) & (cu < chunks))
        def _():
            line(
                cu, z == 0, lambda d: d > z, lambda d: d >= z, up_in, up_out, up_send, up_recv, above
            )

        cd = t - (nz - 1 - z)

        @pl.when((cd >= 0) & (cd < chunks))
        def _():
            line(
                cd, z == nz - 1, lambda d: d < z, lambda d: d <= z, dn_in, dn_out, dn_send, dn_recv, below
            )

        return carry

    lax.fori_loop(0, chunks + nz - 1, tick, 0)

    own = block(z)

    @pl.when(z > 0)
    def _():
        part[own, :] = part[own, :] + up_in[own, :].astype(jnp.float32)

    @pl.when(z < nz - 1)
    def _():
        part[own, :] = part[own, :] + dn_in[own, :].astype(jnp.float32)

    out_ref[...] = (h_ref[...].astype(jnp.float32) + part[own, :]).astype(jnp.bfloat16)

    for d in range(nz):

        @pl.when(d > z)
        def _():
            wait_bytes(up_out.at[pl.ds(d * tok, tok), :], up_send.at[d])

        @pl.when(d < z)
        def _():
            wait_bytes(dn_out.at[pl.ds(d * tok, tok), :], dn_send.at[d])

    def finish(k, carry):
        wait_bytes(r_ref.at[share(lax.rem(me + k, peers)), :], pl_send.at[k])
        return carry

    lax.fori_loop(1, peers, finish, 0)


def routing_tables(packed, nz, nx, ndp, cap, per):
    tok, top = packed.shape[1], packed.shape[2] // 2
    peers = nx * ndp
    sp = lax.axis_index("sp")
    z, x = sp // nx, sp % nx
    packed = lax.dynamic_index_in_dim(packed.reshape(nz, nx, tok, 2 * top), x, 1, keepdims=False)
    chosen = packed[..., :top].astype(jnp.int32)
    experts = z * peers + jnp.arange(peers, dtype=jnp.int32)
    same = chosen[:, :, :, None] == experts
    named = jnp.any(same, axis=2)
    weight = jnp.sum(jnp.where(same, packed[..., top:, None], 0.0), axis=2)
    earlier = jnp.tril(jnp.ones((tok, tok), jnp.bfloat16), -1)
    rank = jnp.einsum(
        "ts,bsp->btp", earlier, named.astype(jnp.bfloat16), preferred_element_type=jnp.float32
    ).astype(jnp.int32)
    slot = jnp.arange(nz, dtype=jnp.int32)[:, None, None] * cap + rank
    slot = jnp.where(named, slot, per)
    slot_ids = jnp.arange(per, dtype=jnp.int32)
    pick = slot.transpose(2, 0, 1)[:, None, :, :] == slot_ids[None, :, None, None]
    pick = pick.astype(jnp.bfloat16).reshape(peers * per, nz * tok)
    mixed = jnp.where(slot[..., None] == slot_ids, weight[..., None], 0.0)
    mixed = mixed.reshape(nz * tok, peers * per)
    high = lax.reduce_precision(mixed, 8, 7)
    return pick, high.astype(jnp.bfloat16), (mixed - high).astype(jnp.bfloat16)


def dispatch(moe_in, pick, w_gate, w_up, nz, nx, ndp, width):
    tok, model = moe_in.shape
    inner = w_gate.shape[1]
    peers = nx * ndp
    total = pick.shape[0]
    chunks = model // width
    bf16 = jnp.bfloat16
    return pl.pallas_call(
        functools.partial(dispatch_kernel, nz, nx, ndp, width),
        out_shape=jax.ShapeDtypeStruct((total, inner), bf16),
        in_specs=[VMEM_WHOLE] * 4,
        out_specs=VMEM_WHOLE,
        scratch_shapes=[
            pltpu.VMEM((nz * tok, model), bf16),
            pltpu.VMEM((total, model), bf16),
            pltpu.VMEM((total, model), bf16),
            pltpu.VMEM((total, inner), jnp.float32),
            pltpu.VMEM((total, inner), jnp.float32),
            pltpu.SemaphoreType.DMA((nz,)),
            pltpu.SemaphoreType.DMA((nz,)),
            pltpu.SemaphoreType.DMA((nz, chunks)),
            pltpu.SemaphoreType.DMA((peers,)),
            pltpu.SemaphoreType.DMA((peers, chunks)),
        ],
        compiler_params=pltpu.CompilerParams(
            collective_id=1, has_side_effects=True, vmem_limit_bytes=60 * 1024 * 1024
        ),
    )(moe_in, pick, w_gate, w_up)


def combine(act, w_down, high, low, hidden, nz, nx, ndp, width):
    tok, model = hidden.shape
    peers = nx * ndp
    total = act.shape[0]
    chunks = model // width
    bf16 = jnp.bfloat16
    return pl.pallas_call(
        functools.partial(return_kernel, nz, nx, ndp, width),
        out_shape=jax.ShapeDtypeStruct((tok, model), bf16),
        in_specs=[VMEM_WHOLE] * 5,
        out_specs=VMEM_WHOLE,
        scratch_shapes=[
            pltpu.VMEM((total, model), bf16),
            pltpu.VMEM((total, model), bf16),
            pltpu.VMEM((nz * tok, model), jnp.float32),
            pltpu.VMEM((nz * tok, model), bf16),
            pltpu.VMEM((nz * tok, model), bf16),
            pltpu.VMEM((nz * tok, model), bf16),
            pltpu.VMEM((nz * tok, model), bf16),
            pltpu.SemaphoreType.DMA((peers,)),
            pltpu.SemaphoreType.DMA((peers, chunks)),
            pltpu.SemaphoreType.DMA((nz,)),
            pltpu.SemaphoreType.DMA((nz,)),
            pltpu.SemaphoreType.DMA((nz, chunks)),
            pltpu.SemaphoreType.DMA((nz, chunks)),
        ],
        compiler_params=pltpu.CompilerParams(
            collective_id=2, has_side_effects=True, vmem_limit_bytes=60 * 1024 * 1024
        ),
    )(act, w_down, high, low, hidden)


def mixer_kernel(
    n,
    q_ref,
    f_ref,
    v_ref,
    og_ref,
    bound_ref,
    gain_ref,
    out_ref,
    qs,
    ks,
    within,
    push,
    keep,
    push_in,
    keep_in,
    before_out,
    before_in,
    push_send,
    keep_send,
    push_recv,
    keep_recv,
    back_send,
    back_recv,
):
    me = lax.axis_index("sp")
    bf16, f32 = jnp.bfloat16, jnp.float32
    tok, _ = q_ref.shape
    heads, size, _ = push.shape
    own = heads // n
    barrier = pltpu.get_barrier_semaphore()

    def other(k):
        return lax.rem(me + k, n)

    def greet_one(k, carry):
        pl.semaphore_signal(barrier, inc=1, device_id={"sp": other(k)}, device_id_type=MESH)
        return carry

    lax.fori_loop(1, n, greet_one, 0)

    row = lax.broadcasted_iota(jnp.int32, (tok, tok), 0)
    col = lax.broadcasted_iota(jnp.int32, (tok, tok), 1)
    causal = row >= col
    lower = jnp.where(causal, 1.0, 0.0).astype(bf16)

    def columns(h):
        return pl.ds(pl.multiple_of(h * size, size), size)

    def group(j):
        return pl.ds(j * own, own)

    def prepare(h, carry):
        cols = columns(h)
        forget = f_ref[:, cols].astype(f32)
        leak = (1.0 - bound_ref[:, cols]) / (1.0 + jnp.exp(forget))
        log_keep = jnp.log1p(-leak)
        first = log_keep.astype(bf16)
        rest = log_keep - first.astype(f32)
        second = rest.astype(bf16)
        third = (rest - second.astype(f32)).astype(bf16)
        log_run = (
            jnp.dot(lower, first, preferred_element_type=f32)
            + jnp.dot(lower, second, preferred_element_type=f32)
            + jnp.dot(lower, third, preferred_element_type=f32)
        )
        last = log_run[tok - 1 : tok, :]
        ks[:, cols] = (leak * jnp.exp(-log_run)).astype(bf16)
        qs[:, cols] = (q_ref[:, cols].astype(f32) * jnp.exp(log_run)).astype(bf16)
        carry_key = (leak * jnp.exp(last - log_run)).astype(bf16)
        push[h] = lax.dot_general(
            v_ref[:, cols], carry_key, (((0,), (0,)), ((), ())), preferred_element_type=f32
        ).astype(bf16)
        keep[h] = jnp.broadcast_to(jnp.exp(last), (8, size))
        return carry

    lax.fori_loop(0, heads, prepare, 0)
    pl.semaphore_wait(barrier, n - 1)

    def send_push(k, carry):
        j = other(k)
        pltpu.make_async_remote_copy(
            src_ref=push.at[group(j)],
            dst_ref=push_in.at[group(me)],
            send_sem=push_send.at[k],
            recv_sem=push_recv.at[me],
            device_id={"sp": j},
            device_id_type=MESH,
        ).start()
        pltpu.make_async_remote_copy(
            src_ref=keep.at[group(j)],
            dst_ref=keep_in.at[group(me)],
            send_sem=keep_send.at[k],
            recv_sem=keep_recv.at[me],
            device_id={"sp": j},
            device_id_type=MESH,
        ).start()
        return carry

    lax.fori_loop(1, n, send_push, 0)
    push_in[group(me)] = push[group(me)]
    keep_in[group(me)] = keep[group(me)]

    def inside(h, carry):
        cols = columns(h)
        scores = lax.dot_general(
            qs[:, cols], ks[:, cols], (((1,), (1,)), ((), ())), preferred_element_type=f32
        )
        scores = jnp.where(causal, scores, 0.0).astype(bf16)
        within[:, cols] = jnp.dot(scores, v_ref[:, cols], preferred_element_type=f32)
        return carry

    lax.fori_loop(0, heads, inside, 0)

    def scan(b, states):
        @pl.when(b != me)
        def _():
            wait_bytes(push_in.at[group(b)], push_recv.at[b])
            wait_bytes(keep_in.at[group(b)], keep_recv.at[b])

        for i in range(own):
            before_out[b * own + i] = states[i].astype(bf16)

        @pl.when(b != me)
        def _():
            pltpu.make_async_remote_copy(
                src_ref=before_out.at[group(b)],
                dst_ref=before_in.at[group(me)],
                send_sem=back_send.at[b],
                recv_sem=back_recv.at[me],
                device_id={"sp": b},
                device_id_type=MESH,
            ).start()

        @pl.when(b == me)
        def _():
            before_in[group(me)] = before_out[group(me)]

        return tuple(
            states[i] * keep_in[b * own + i][0:1, :] + push_in[b * own + i].astype(f32)
            for i in range(own)
        )

    lax.fori_loop(0, n, scan, tuple(jnp.zeros((size, size), f32) for _ in range(own)))

    def settle(k, carry):
        j = other(k)
        wait_bytes(before_in.at[group(j)], back_recv.at[j])
        return carry

    lax.fori_loop(1, n, settle, 0)

    def close(h, carry):
        cols = columns(h)
        mix = within[:, cols] + lax.dot_general(
            qs[:, cols], before_in[h], (((1,), (1,)), ((), ())), preferred_element_type=f32
        )
        scale = lax.rsqrt(jnp.mean(mix * mix, axis=-1, keepdims=True) + NORM_EPS)
        normed = (mix * scale * gain_ref[...]).astype(bf16).astype(f32)
        gate = og_ref[:, cols].astype(f32)
        out_ref[:, cols] = (normed * (gate / (1.0 + jnp.exp(-gate)))).astype(bf16)
        return carry

    lax.fori_loop(0, heads, close, 0)

    def finish(k, carry):
        j = other(k)
        wait_bytes(push.at[group(j)], push_send.at[k])
        wait_bytes(keep.at[group(j)], keep_send.at[k])
        wait_bytes(before_out.at[group(j)], back_send.at[j])
        return carry

    lax.fori_loop(1, n, finish, 0)


def mixer(q, f, v, og, bound, gain):
    n = lax.axis_size("sp")
    tok, wide = q.shape
    size = gain.shape[1]
    heads = wide // size
    bf16 = jnp.bfloat16
    states = pltpu.VMEM((heads, size, size), bf16)
    keeps = pltpu.VMEM((heads, 8, size), jnp.float32)
    return pl.pallas_call(
        functools.partial(mixer_kernel, n),
        out_shape=jax.ShapeDtypeStruct((tok, wide), bf16),
        in_specs=[VMEM_WHOLE] * 6,
        out_specs=VMEM_WHOLE,
        scratch_shapes=[
            pltpu.VMEM((tok, wide), bf16),
            pltpu.VMEM((tok, wide), bf16),
            pltpu.VMEM((tok, wide), jnp.float32),
            states,
            keeps,
            states,
            keeps,
            states,
            states,
        ]
        + [pltpu.SemaphoreType.DMA((n,))] * 6,
        compiler_params=pltpu.CompilerParams(
            collective_id=3, has_side_effects=True, vmem_limit_bytes=32 * 1024 * 1024
        ),
    )(q, f, v, og, bound, gain)


def project_kernel(
    ndp,
    parts,
    g_ref,
    w_ref,
    res_ref,
    gain_ref,
    hid_ref,
    moe_ref,
    g_in,
    outs,
    proj,
    far_send,
    near_send,
    relay_send,
    g_recv,
    r_send,
    r_recv,
):
    me = lax.axis_index("dp")
    tok, wide = g_ref.shape
    share = w_ref.shape[1]
    ny = ndp // 2
    y, core = lax.div(me, 2), lax.rem(me, 2)
    partner = y * 2 + 1 - core
    piece = wide // parts
    barrier = pltpu.get_barrier_semaphore()
    for k in range(1, ndp):
        pl.semaphore_signal(
            barrier, inc=1, device_id={"dp": lax.rem(me + k, ndp)}, device_id_type=MESH
        )
    pl.semaphore_wait(barrier, ndp - 1)

    def rows(j):
        return pl.ds(pl.multiple_of(j * tok, tok), tok)

    def span(c):
        return pl.ds(c * piece, piece)

    def send(src, owner, c, sem, target):
        pltpu.make_async_remote_copy(
            src_ref=src,
            dst_ref=g_in.at[rows(owner), span(c)],
            send_sem=sem,
            recv_sem=g_recv.at[owner, c],
            device_id={"dp": target},
            device_id_type=MESH,
        ).start()

    for c in range(parts):
        for k in range(1, ny):
            send(g_ref.at[:, span(c)], me, c, far_send.at[k], lax.rem(y + k, ny) * 2 + core)
        send(g_ref.at[:, span(c)], me, c, near_send, partner)

    def arrive(owner, c):
        wait_bytes(g_in.at[rows(owner), span(c)], g_recv.at[owner, c])

    mine = pl.ds(pl.multiple_of(me * share, share), share)

    def multiply(src, owner):
        def tile(i, carry):
            cols = pl.ds(pl.multiple_of(i * 256, 256), 256)
            outs[rows(owner), cols] = jnp.dot(
                src[...], w_ref[:, cols], preferred_element_type=jnp.float32
            ).astype(jnp.bfloat16)
            return carry

        lax.fori_loop(0, share // 256, tile, 0)

    def answer(owner):
        multiply(g_in.at[rows(owner), :], owner)
        pltpu.make_async_remote_copy(
            src_ref=outs.at[rows(owner), :],
            dst_ref=proj.at[:, mine],
            send_sem=r_send.at[owner],
            recv_sem=r_recv.at[me],
            device_id={"dp": owner},
            device_id_type=MESH,
        ).start()

    multiply(g_ref, me)
    proj[:, mine] = outs[rows(me), :]

    for c in range(parts):
        arrive(partner, c)
    answer(partner)

    def source(k):
        return lax.rem(y + ny - k, ny) * 2

    for c in range(parts):
        for k in range(1, ny):
            owner = source(k) + core
            arrive(owner, c)
            send(g_in.at[rows(owner), span(c)], owner, c, relay_send.at[k], partner)
    for k in range(1, ny):
        answer(source(k) + core)
    for k in range(1, ny):
        owner = source(k) + 1 - core
        for c in range(parts):
            arrive(owner, c)
        answer(owner)
    for k in range(1, ndp):
        owner = lax.rem(me + k, ndp)
        cols = pl.ds(pl.multiple_of(owner * share, share), share)
        wait_bytes(proj.at[:, cols], r_recv.at[owner])
    hidden = (res_ref[...].astype(jnp.float32) + proj[...].astype(jnp.float32)).astype(jnp.bfloat16)
    hid_ref[...] = hidden
    hidden_f = hidden.astype(jnp.float32)
    scale = lax.rsqrt(jnp.mean(hidden_f * hidden_f, axis=-1, keepdims=True) + NORM_EPS)
    moe_ref[...] = (hidden_f * scale * gain_ref[...]).astype(jnp.bfloat16)
    for k in range(1, ny):
        wait_bytes(g_ref, far_send.at[k])
        wait_bytes(g_ref, relay_send.at[k])
    wait_bytes(g_ref, near_send)
    for k in range(1, ndp):
        owner = lax.rem(me + k, ndp)
        wait_bytes(outs.at[rows(owner), :], r_send.at[owner])


def project(gated, weight, residual, gain):
    ndp = lax.axis_size("dp")
    tok, wide = gated.shape
    share = weight.shape[1]
    model = residual.shape[1]
    bf16 = jnp.bfloat16
    dma = pltpu.SemaphoreType.DMA
    return pl.pallas_call(
        functools.partial(project_kernel, ndp, GATED_PARTS),
        out_shape=[jax.ShapeDtypeStruct((tok, model), bf16)] * 2,
        in_specs=[VMEM_WHOLE] * 4,
        out_specs=[VMEM_WHOLE] * 2,
        scratch_shapes=[
            pltpu.VMEM((ndp * tok, wide), bf16),
            pltpu.VMEM((ndp * tok, share), bf16),
            pltpu.VMEM((tok, model), bf16),
            dma((ndp,)),
            dma,
            dma((ndp,)),
            dma((ndp, GATED_PARTS)),
            dma((ndp,)),
            dma((ndp,)),
        ],
        compiler_params=pltpu.CompilerParams(
            collective_id=4, has_side_effects=True, vmem_limit_bytes=32 * 1024 * 1024
        ),
    )(gated, weight, residual, gain)


def local(
    queries,
    forget_pre,
    values,
    out_gate,
    lower_bound,
    head_gain,
    residual,
    out_weight,
    ffn_gain,
    routing,
    route_weight,
    expert_gate,
    expert_up,
    expert_down,
):
    _, tok_rows, channels = queries.shape
    model_width = residual.shape[2]
    top_count = routing.shape[2]
    span_sp = lax.axis_size("sp")
    span_dp = lax.axis_size("dp")
    experts = expert_gate.shape[0] * span_sp * span_dp
    cap = max(2, 5 * tok_rows * top_count // (4 * experts))
    nx = span_dp // 2
    nz = span_sp // nx
    per = -(-nz * cap // 16) * 16
    width = min(CHUNK, model_width)
    packed = jnp.concatenate(
        [routing.astype(jnp.float32), route_weight], axis=2
    ).reshape(tok_rows * 2 * top_count)
    shared = lax.all_gather(jnp.concatenate([packed, lower_bound]), "sp", axis=0)
    packed, bound = shared[:, : packed.shape[0]], shared[:, packed.shape[0] :]
    gated = mixer(
        queries[0],
        forget_pre[0],
        values[0],
        out_gate[0],
        bound.reshape(1, channels),
        head_gain[None, :],
    )
    hidden, moe_in = project(gated, out_weight, residual[0], ffn_gain[None, :])
    pick, high, low = routing_tables(
        packed.reshape(span_sp, tok_rows, 2 * top_count),
        nz,
        nx,
        span_dp,
        cap,
        per,
    )
    act = dispatch(moe_in, pick, expert_gate[0], expert_up[0], nz, nx, span_dp, width)
    layer_out = combine(act, expert_down[0], high, low, hidden, nz, nx, span_dp, width)
    return layer_out.reshape(1, tok_rows, model_width)


def solution(mesh):
    in_specs = (
        P("dp", "sp", None),
        P("dp", "sp", None),
        P("dp", "sp", None),
        P("dp", "sp", None),
        P("sp"),
        P(),
        P("dp", "sp", None),
        P(None, "dp"),
        P(),
        P("dp", "sp", None),
        P("dp", "sp", None),
        P(("sp", "dp"), None, None),
        P(("sp", "dp"), None, None),
        P(("sp", "dp"), None, None),
    )
    out_specs = P("dp", "sp", None)
    return jax.shard_map(local, mesh=mesh, in_specs=in_specs, out_specs=out_specs, check_vma=False)
```

```python
import functools

import jax
import jax.numpy as jnp
from jax import lax
from jax.experimental import pallas as pl
from jax.experimental.pallas import tpu as pltpu
from jax.sharding import PartitionSpec as P

MESH = pl.DeviceIdType.MESH
VMEM_WHOLE = pl.BlockSpec(memory_space=pltpu.VMEM)

CHUNK = 256
GATED_PARTS = 4


NORM_EPS = 1e-06


def wait_bytes(ref, sem):
    pltpu.make_async_copy(ref, ref, sem).wait()


def place(nz, nx, ndp):
    sp, dp = lax.axis_index("sp"), lax.axis_index("dp")
    z = lax.div(sp, nx)
    me = lax.rem(sp, nx) * ndp + dp
    above, below = {"sp": sp + nx, "dp": dp}, {"sp": sp - nx, "dp": dp}

    def member(p):
        return {"sp": z * nx + lax.div(p, ndp), "dp": lax.rem(p, ndp)}

    return z, me, above, below, member


def greet(nz, peers, z, me, above, below, member):
    barrier = pltpu.get_barrier_semaphore()

    @pl.when(z > 0)
    def _():
        pl.semaphore_signal(barrier, inc=1, device_id=below, device_id_type=MESH)

    @pl.when(z < nz - 1)
    def _():
        pl.semaphore_signal(barrier, inc=1, device_id=above, device_id_type=MESH)

    def one(k, carry):
        pl.semaphore_signal(
            barrier, inc=1, device_id=member(lax.rem(me + k, peers)), device_id_type=MESH
        )
        return carry

    lax.fori_loop(1, peers, one, 0)
    count = peers - 1 + jnp.where(z > 0, 1, 0) + jnp.where(z < nz - 1, 1, 0)
    pl.semaphore_wait(barrier, count)


def routing_tables(packed_ref, nz, nx, ndp, cap):
    peers = nx * ndp
    _, double, tok = packed_ref.shape
    top = double // 2
    sp = lax.axis_index("sp")
    z, x = lax.div(sp, nx), lax.rem(sp, nx)
    ids = lax.broadcasted_iota(jnp.int32, (peers, tok), 0) + z * peers
    row = lax.broadcasted_iota(jnp.int32, (tok, tok), 0)
    col = lax.broadcasted_iota(jnp.int32, (tok, tok), 1)
    earlier = jnp.where(row < col, 1.0, 0.0).astype(jnp.bfloat16)
    found = []
    for b in range(nz):
        item = packed_ref[b * nx + x]
        chosen = item[:top].astype(jnp.int32)
        named = jnp.zeros((peers, tok), jnp.float32)
        weight = jnp.zeros((peers, tok), jnp.float32)
        for j in range(top):
            same = chosen[j : j + 1] == ids
            named = jnp.where(same, 1.0, named)
            weight = jnp.where(same, item[top + j : top + j + 1], weight)
        rank = jnp.dot(named.astype(jnp.bfloat16), earlier, preferred_element_type=jnp.float32)
        slot = jnp.where(named > 0, b * cap + rank.astype(jnp.int32), -1)
        found.append((slot, weight))
    return found


def dispatch_kernel(
    nz,
    nx,
    ndp,
    width,
    cap,
    x_ref,
    packed_ref,
    gate_ref,
    lift_ref,
    act_ref,
    pick_ref,
    gath,
    slots,
    got,
    gate_sum,
    lift_sum,
    up_send,
    dn_send,
    line_recv,
    pl_send,
    pl_recv,
):
    peers = nx * ndp
    z, me, above, below, member = place(nz, nx, ndp)
    tok, model = x_ref.shape
    chunks = model // width
    per = act_ref.shape[0] // peers
    greet(nz, peers, z, me, above, below, member)

    def block(b):
        return pl.ds(pl.multiple_of(b * tok, tok), tok)

    def share(p):
        return pl.ds(pl.multiple_of(p * per, per), per)

    def pass_on(src, b, c, cols, sem, device):
        pltpu.make_async_remote_copy(
            src_ref=src,
            dst_ref=gath.at[block(b), cols],
            send_sem=sem,
            recv_sem=line_recv.at[b, c],
            device_id=device,
            device_id_type=MESH,
        ).start()

    gath[block(z), :] = x_ref[...]
    slot_ids = lax.broadcasted_iota(jnp.int32, (per, tok), 0)
    for b, (slot, _) in enumerate(routing_tables(packed_ref, nz, nx, ndp, cap)):
        for p in range(peers):
            pick_ref[p * per : (p + 1) * per, b * tok : (b + 1) * tok] = jnp.where(
                slot_ids == slot[p : p + 1], 1.0, 0.0
            ).astype(jnp.bfloat16)
    gate_sum[...] = jnp.zeros_like(gate_sum)
    lift_sum[...] = jnp.zeros_like(lift_sum)

    def tick(t, carry):
        for s in range(nz):
            c = t - s
            cols = pl.ds(pl.multiple_of(c * width, width), width)
            valid = (c >= 0) & (c < chunks)
            if s == 0:

                @pl.when(valid & (z < nz - 1))
                def _():
                    pass_on(x_ref.at[:, cols], z, c, cols, up_send.at[0], above)

                @pl.when(valid & (z > 0))
                def _():
                    pass_on(x_ref.at[:, cols], z, c, cols, dn_send.at[0], below)

                continue

            @pl.when(valid & (z - s >= 0))
            def _():
                b = z - s
                here = gath.at[block(b), cols]
                wait_bytes(here, line_recv.at[b, c])

                @pl.when(z < nz - 1)
                def _():
                    pass_on(here, b, c, cols, up_send.at[s], above)

            @pl.when(valid & (z + s < nz))
            def _():
                b = z + s
                here = gath.at[block(b), cols]
                wait_bytes(here, line_recv.at[b, c])

                @pl.when(z > 0)
                def _():
                    pass_on(here, b, c, cols, dn_send.at[s], below)

        c = t - (nz - 1)

        @pl.when((c >= 0) & (c < chunks))
        def _():
            cols = pl.ds(pl.multiple_of(c * width, width), width)
            slots[:, cols] = jnp.dot(
                pick_ref[...], gath[:, cols], preferred_element_type=jnp.float32
            ).astype(jnp.bfloat16)
            got[share(me), cols] = slots[share(me), cols]

            def send(k, inner):
                p = lax.rem(me + k, peers)
                pltpu.make_async_remote_copy(
                    src_ref=slots.at[share(p), cols],
                    dst_ref=got.at[share(me), cols],
                    send_sem=pl_send.at[k],
                    recv_sem=pl_recv.at[k, c],
                    device_id=member(p),
                    device_id_type=MESH,
                ).start()
                return inner

            lax.fori_loop(1, peers, send, 0)

        late = t - nz

        @pl.when(late >= 0)
        def _():
            cols = pl.ds(pl.multiple_of(late * width, width), width)

            def arrive(k, inner):
                p = lax.rem(me + peers - k, peers)
                wait_bytes(got.at[share(p), cols], pl_recv.at[k, late])
                return inner

            lax.fori_loop(1, peers, arrive, 0)
            rows = got[:, cols]
            gate_sum[...] += jnp.dot(rows, gate_ref[cols, :], preferred_element_type=jnp.float32)
            lift_sum[...] += jnp.dot(rows, lift_ref[cols, :], preferred_element_type=jnp.float32)

        return carry

    lax.fori_loop(0, chunks + nz, tick, 0)
    gate = gate_sum[...]
    act_ref[...] = (gate / (1.0 + jnp.exp(-gate)) * lift_sum[...]).astype(jnp.bfloat16)

    for s in range(nz - 1):

        @pl.when((z - s >= 0) & (z < nz - 1))
        def _():
            wait_bytes(x_ref, up_send.at[s])

        @pl.when((z + s < nz) & (z > 0))
        def _():
            wait_bytes(x_ref, dn_send.at[s])

    def finish(k, carry):
        wait_bytes(slots.at[share(lax.rem(me + k, peers)), :], pl_send.at[k])
        return carry

    lax.fori_loop(1, peers, finish, 0)


def return_kernel(
    nz,
    nx,
    ndp,
    width,
    cap,
    act_ref,
    down_ref,
    packed_ref,
    h_ref,
    out_ref,
    mixed,
    high_ref,
    low_ref,
    r_ref,
    ret,
    part,
    up_out,
    up_in,
    dn_out,
    dn_in,
    pl_send,
    pl_recv,
    up_send,
    dn_send,
    up_recv,
    dn_recv,
):
    peers = nx * ndp
    z, me, above, below, member = place(nz, nx, ndp)
    tok, model = h_ref.shape
    chunks = model // width
    per = r_ref.shape[0] // peers
    greet(nz, peers, z, me, above, below, member)

    def block(b):
        return pl.ds(pl.multiple_of(b * tok, tok), tok)

    def share(p):
        return pl.ds(pl.multiple_of(p * per, per), per)

    def columns(c):
        return pl.ds(pl.multiple_of(c * width, width), width)

    def send_chunk(c, carry):
        r_ref[:, columns(c)] = jnp.dot(
            act_ref[...], down_ref[:, columns(c)], preferred_element_type=jnp.float32
        ).astype(jnp.bfloat16)

        def send(k, inner):
            p = lax.rem(me + k, peers)
            pltpu.make_async_remote_copy(
                src_ref=r_ref.at[share(p), columns(c)],
                dst_ref=ret.at[share(me), columns(c)],
                send_sem=pl_send.at[k],
                recv_sem=pl_recv.at[k, c],
                device_id=member(p),
                device_id_type=MESH,
            ).start()
            return inner

        return lax.fori_loop(1, peers, send, carry)

    lax.fori_loop(0, chunks, send_chunk, 0)
    ret[share(me), :] = r_ref[share(me), :]
    slot_ids = lax.broadcasted_iota(jnp.int32, (per, tok), 0)
    for b, (slot, weight) in enumerate(routing_tables(packed_ref, nz, nx, ndp, cap)):
        for p in range(peers):
            mixed[p * per : (p + 1) * per, b * tok : (b + 1) * tok] = jnp.where(
                slot_ids == slot[p : p + 1], weight[p : p + 1], 0.0
            )
    turned = mixed[...].T
    high = turned.astype(jnp.bfloat16)
    high_ref[...] = high
    low_ref[...] = (turned - high.astype(jnp.float32)).astype(jnp.bfloat16)

    def line(order, c, first, sends, takes, inbox, outbox, send_sem, recv_sem, device):
        cols = columns(c)
        for d in order:
            rows = pl.ds(d * tok, tok)

            @pl.when(jnp.logical_not(first) & takes(d))
            def _():
                wait_bytes(inbox.at[rows, cols], recv_sem.at[d, c])

            @pl.when(sends(d))
            def _():
                @pl.when(first)
                def _():
                    outbox[rows, cols] = part[rows, cols].astype(jnp.bfloat16)

                @pl.when(jnp.logical_not(first))
                def _():
                    outbox[rows, cols] = (
                        part[rows, cols] + inbox[rows, cols].astype(jnp.float32)
                    ).astype(jnp.bfloat16)

                pltpu.make_async_remote_copy(
                    src_ref=outbox.at[rows, cols],
                    dst_ref=inbox.at[rows, cols],
                    send_sem=send_sem.at[d],
                    recv_sem=recv_sem.at[d, c],
                    device_id=device,
                    device_id_type=MESH,
                ).start()

    def tick(t, carry):
        @pl.when(t < chunks)
        def _():
            cols = columns(t)

            def arrive(k, inner):
                p = lax.rem(me + peers - k, peers)
                wait_bytes(ret.at[share(p), cols], pl_recv.at[k, t])
                return inner

            lax.fori_loop(1, peers, arrive, 0)
            rows = ret[:, cols]
            part[:, cols] = jnp.dot(
                high_ref[...], rows, preferred_element_type=jnp.float32
            ) + jnp.dot(low_ref[...], rows, preferred_element_type=jnp.float32)

        cu = t - z

        @pl.when((cu >= 0) & (cu < chunks))
        def _():
            line(
                range(nz - 1, -1, -1),
                cu,
                z == 0,
                lambda d: d > z,
                lambda d: d >= z,
                up_in,
                up_out,
                up_send,
                up_recv,
                above,
            )

        cd = t - (nz - 1 - z)

        @pl.when((cd >= 0) & (cd < chunks))
        def _():
            line(
                range(nz),
                cd,
                z == nz - 1,
                lambda d: d < z,
                lambda d: d <= z,
                dn_in,
                dn_out,
                dn_send,
                dn_recv,
                below,
            )

        return carry

    lax.fori_loop(0, chunks + nz - 1, tick, 0)

    own = block(z)

    @pl.when(z > 0)
    def _():
        part[own, :] = part[own, :] + up_in[own, :].astype(jnp.float32)

    @pl.when(z < nz - 1)
    def _():
        part[own, :] = part[own, :] + dn_in[own, :].astype(jnp.float32)

    out_ref[...] = (h_ref[...].astype(jnp.float32) + part[own, :]).astype(jnp.bfloat16)

    for d in range(nz):

        @pl.when(d > z)
        def _():
            wait_bytes(up_out.at[pl.ds(d * tok, tok), :], up_send.at[d])

        @pl.when(d < z)
        def _():
            wait_bytes(dn_out.at[pl.ds(d * tok, tok), :], dn_send.at[d])

    def finish(k, carry):
        wait_bytes(r_ref.at[share(lax.rem(me + k, peers)), :], pl_send.at[k])
        return carry

    lax.fori_loop(1, peers, finish, 0)


def dispatch(moe_in, packed, w_gate, w_up, nz, nx, ndp, width, cap, per):
    tok, model = moe_in.shape
    inner = w_gate.shape[1]
    peers = nx * ndp
    total = peers * per
    chunks = model // width
    bf16 = jnp.bfloat16
    return pl.pallas_call(
        functools.partial(dispatch_kernel, nz, nx, ndp, width, cap),
        out_shape=jax.ShapeDtypeStruct((total, inner), bf16),
        in_specs=[VMEM_WHOLE] * 4,
        out_specs=VMEM_WHOLE,
        scratch_shapes=[
            pltpu.VMEM((total, nz * tok), bf16),
            pltpu.VMEM((nz * tok, model), bf16),
            pltpu.VMEM((total, model), bf16),
            pltpu.VMEM((total, model), bf16),
            pltpu.VMEM((total, inner), jnp.float32),
            pltpu.VMEM((total, inner), jnp.float32),
            pltpu.SemaphoreType.DMA((nz,)),
            pltpu.SemaphoreType.DMA((nz,)),
            pltpu.SemaphoreType.DMA((nz, chunks)),
            pltpu.SemaphoreType.DMA((peers,)),
            pltpu.SemaphoreType.DMA((peers, chunks)),
        ],
        compiler_params=pltpu.CompilerParams(
            collective_id=1, has_side_effects=True, vmem_limit_bytes=60 * 1024 * 1024
        ),
    )(moe_in, packed, w_gate, w_up)


def combine(act, w_down, packed, hidden, nz, nx, ndp, width, cap):
    tok, model = hidden.shape
    peers = nx * ndp
    total = act.shape[0]
    chunks = model // width
    bf16 = jnp.bfloat16
    return pl.pallas_call(
        functools.partial(return_kernel, nz, nx, ndp, width, cap),
        out_shape=jax.ShapeDtypeStruct((tok, model), bf16),
        in_specs=[VMEM_WHOLE] * 4,
        out_specs=VMEM_WHOLE,
        scratch_shapes=[
            pltpu.VMEM((total, nz * tok), jnp.float32),
            pltpu.VMEM((nz * tok, total), bf16),
            pltpu.VMEM((nz * tok, total), bf16),
            pltpu.VMEM((total, model), bf16),
            pltpu.VMEM((total, model), bf16),
            pltpu.VMEM((nz * tok, model), jnp.float32),
            pltpu.VMEM((nz * tok, model), bf16),
            pltpu.VMEM((nz * tok, model), bf16),
            pltpu.VMEM((nz * tok, model), bf16),
            pltpu.VMEM((nz * tok, model), bf16),
            pltpu.SemaphoreType.DMA((peers,)),
            pltpu.SemaphoreType.DMA((peers, chunks)),
            pltpu.SemaphoreType.DMA((nz,)),
            pltpu.SemaphoreType.DMA((nz,)),
            pltpu.SemaphoreType.DMA((nz, chunks)),
            pltpu.SemaphoreType.DMA((nz, chunks)),
        ],
        compiler_params=pltpu.CompilerParams(
            collective_id=2, has_side_effects=True, vmem_limit_bytes=60 * 1024 * 1024
        ),
    )(act, w_down, packed, hidden)


def mixer_kernel(
    n,
    q_ref,
    f_ref,
    v_ref,
    og_ref,
    own_bound_ref,
    own_pack_ref,
    gain_ref,
    out_ref,
    pack_ref,
    bound_in,
    qs,
    qr,
    ks,
    kr,
    within,
    push,
    keep,
    push_in,
    keep_in,
    before_out,
    before_in,
    bound_send,
    pack_send,
    bound_recv,
    pack_recv,
    push_send,
    keep_send,
    push_recv,
    keep_recv,
    back_send,
    back_recv,
):
    me = lax.axis_index("sp")
    bf16, f32 = jnp.bfloat16, jnp.float32
    tok, _ = q_ref.shape
    heads, size, _ = push.shape
    own = heads // n
    barrier = pltpu.get_barrier_semaphore()

    def other(k):
        return lax.rem(me + k, n)

    def greet_one(k, carry):
        pl.semaphore_signal(barrier, inc=1, device_id={"sp": other(k)}, device_id_type=MESH)
        return carry

    lax.fori_loop(1, n, greet_one, 0)

    bound_in[me] = own_bound_ref[...]
    pack_ref[me] = own_pack_ref[...]
    pl.semaphore_wait(barrier, n - 1)

    def spread(k, carry):
        for src, dst, send_sem, recv_sem in (
            (own_bound_ref, bound_in, bound_send, bound_recv),
            (own_pack_ref, pack_ref, pack_send, pack_recv),
        ):
            pltpu.make_async_remote_copy(
                src_ref=src,
                dst_ref=dst.at[me],
                send_sem=send_sem.at[k],
                recv_sem=recv_sem.at[me],
                device_id={"sp": other(k)},
                device_id_type=MESH,
            ).start()
        return carry

    lax.fori_loop(1, n, spread, 0)

    row = lax.broadcasted_iota(jnp.int32, (tok, tok), 0)
    col = lax.broadcasted_iota(jnp.int32, (tok, tok), 1)
    causal = row >= col
    lower = jnp.where(causal, 1.0, 0.0).astype(bf16)

    def columns(h):
        return pl.ds(pl.multiple_of(h * size, size), size)

    def group(j):
        return pl.ds(j * own, own)

    def halves(value):
        first = value.astype(bf16)
        return first, (value - first.astype(f32)).astype(bf16)

    def prepare(j, carry):
        @pl.when(j != me)
        def _():
            wait_bytes(bound_in.at[j], bound_recv.at[j])

        for i in range(own):
            h = j * own + i
            cols = columns(h)
            bound = bound_in[j][:, i * size : (i + 1) * size]
            forget = f_ref[:, cols].astype(f32)
            leak = (1.0 - bound) / (1.0 + jnp.exp(forget))
            log_keep = jnp.log1p(-leak)
            first = log_keep.astype(bf16)
            second, third = halves(log_keep - first.astype(f32))
            log_run = (
                jnp.dot(lower, first, preferred_element_type=f32)
                + jnp.dot(lower, second, preferred_element_type=f32)
                + jnp.dot(lower, third, preferred_element_type=f32)
            )
            last = log_run[tok - 1 : tok, :]
            ks[:, cols], kr[:, cols] = halves(leak * jnp.exp(-log_run))
            qs[:, cols], qr[:, cols] = halves(q_ref[:, cols].astype(f32) * jnp.exp(log_run))
            total = jnp.zeros((size, size), f32)
            for term in halves(leak * jnp.exp(last - log_run)):
                total = total + lax.dot_general(
                    v_ref[:, cols], term, (((0,), (0,)), ((), ())), preferred_element_type=f32
                )
            push[h] = total.astype(bf16)
            keep[h] = jnp.broadcast_to(jnp.exp(last), (8, size))
        return carry

    lax.fori_loop(0, n, prepare, 0)

    def send_push(k, carry):
        j = other(k)
        pltpu.make_async_remote_copy(
            src_ref=push.at[group(j)],
            dst_ref=push_in.at[group(me)],
            send_sem=push_send.at[k],
            recv_sem=push_recv.at[me],
            device_id={"sp": j},
            device_id_type=MESH,
        ).start()
        pltpu.make_async_remote_copy(
            src_ref=keep.at[group(j)],
            dst_ref=keep_in.at[group(me)],
            send_sem=keep_send.at[k],
            recv_sem=keep_recv.at[me],
            device_id={"sp": j},
            device_id_type=MESH,
        ).start()
        return carry

    lax.fori_loop(1, n, send_push, 0)
    push_in[group(me)] = push[group(me)]
    keep_in[group(me)] = keep[group(me)]

    def across(a, b):
        return lax.dot_general(a, b, (((1,), (1,)), ((), ())), preferred_element_type=f32)

    def inside(j, carry):
        for i in range(own):
            cols = columns(j * own + i)
            scores = (
                across(qs[:, cols], ks[:, cols])
                + across(qs[:, cols], kr[:, cols])
                + across(qr[:, cols], ks[:, cols])
            )
            first, second = halves(jnp.where(causal, scores, 0.0))
            within[:, cols] = jnp.dot(
                first, v_ref[:, cols], preferred_element_type=f32
            ) + jnp.dot(second, v_ref[:, cols], preferred_element_type=f32)
        return carry

    lax.fori_loop(0, n, inside, 0)

    def scan(b, states):
        @pl.when(b != me)
        def _():
            wait_bytes(push_in.at[group(b)], push_recv.at[b])
            wait_bytes(keep_in.at[group(b)], keep_recv.at[b])

        for i in range(own):
            before_out[b * own + i] = states[i].astype(bf16)

        @pl.when(b != me)
        def _():
            pltpu.make_async_remote_copy(
                src_ref=before_out.at[group(b)],
                dst_ref=before_in.at[group(me)],
                send_sem=back_send.at[b],
                recv_sem=back_recv.at[me],
                device_id={"sp": b},
                device_id_type=MESH,
            ).start()

        @pl.when(b == me)
        def _():
            before_in[group(me)] = before_out[group(me)]

        return tuple(
            states[i] * keep_in[b * own + i][0:1, :] + push_in[b * own + i].astype(f32)
            for i in range(own)
        )

    lax.fori_loop(0, n, scan, tuple(jnp.zeros((size, size), f32) for _ in range(own)))

    def settle(k, carry):
        j = other(k)
        wait_bytes(before_in.at[group(j)], back_recv.at[j])
        return carry

    lax.fori_loop(1, n, settle, 0)

    def close(j, carry):
        for i in range(own):
            h = j * own + i
            cols = columns(h)
            mix = (
                within[:, cols]
                + across(qs[:, cols], before_in[h])
                + across(qr[:, cols], before_in[h])
            )
            scale = lax.rsqrt(jnp.mean(mix * mix, axis=-1, keepdims=True) + NORM_EPS)
            normed = (mix * scale * gain_ref[...]).astype(bf16).astype(f32)
            gate = og_ref[:, cols].astype(f32)
            out_ref[:, cols] = (normed * (gate / (1.0 + jnp.exp(-gate)))).astype(bf16)
        return carry

    lax.fori_loop(0, n, close, 0)

    def finish(k, carry):
        j = other(k)
        wait_bytes(pack_ref.at[j], pack_recv.at[j])
        wait_bytes(own_pack_ref, pack_send.at[k])
        wait_bytes(own_bound_ref, bound_send.at[k])
        wait_bytes(push.at[group(j)], push_send.at[k])
        wait_bytes(keep.at[group(j)], keep_send.at[k])
        wait_bytes(before_out.at[group(j)], back_send.at[j])
        return carry

    lax.fori_loop(1, n, finish, 0)


def mixer(q, f, v, og, bound, pack, gain):
    n = lax.axis_size("sp")
    tok, wide = q.shape
    size = gain.shape[1]
    heads = wide // size
    bf16 = jnp.bfloat16
    states = pltpu.VMEM((heads, size, size), bf16)
    keeps = pltpu.VMEM((heads, 8, size), jnp.float32)
    return pl.pallas_call(
        functools.partial(mixer_kernel, n),
        out_shape=[
            jax.ShapeDtypeStruct((tok, wide), bf16),
            jax.ShapeDtypeStruct((n,) + pack.shape, jnp.float32),
        ],
        in_specs=[VMEM_WHOLE] * 7,
        out_specs=[VMEM_WHOLE] * 2,
        scratch_shapes=[
            pltpu.VMEM((n,) + bound.shape, jnp.float32),
            pltpu.VMEM((tok, wide), bf16),
            pltpu.VMEM((tok, wide), bf16),
            pltpu.VMEM((tok, wide), bf16),
            pltpu.VMEM((tok, wide), bf16),
            pltpu.VMEM((tok, wide), jnp.float32),
            states,
            keeps,
            states,
            keeps,
            states,
            states,
        ]
        + [pltpu.SemaphoreType.DMA((n,))] * 10,
        compiler_params=pltpu.CompilerParams(
            collective_id=3, has_side_effects=True, vmem_limit_bytes=32 * 1024 * 1024
        ),
    )(q, f, v, og, bound, pack, gain)


def project_kernel(
    ndp,
    parts,
    g_ref,
    w_ref,
    res_ref,
    gain_ref,
    hid_ref,
    moe_ref,
    g_in,
    outs,
    proj,
    far_send,
    near_send,
    relay_send,
    g_recv,
    r_send,
    r_recv,
):
    me = lax.axis_index("dp")
    tok, wide = g_ref.shape
    share = w_ref.shape[1]
    ny = ndp // 2
    y, core = lax.div(me, 2), lax.rem(me, 2)
    partner = y * 2 + 1 - core
    piece = wide // parts
    barrier = pltpu.get_barrier_semaphore()
    for k in range(1, ndp):
        pl.semaphore_signal(
            barrier, inc=1, device_id={"dp": lax.rem(me + k, ndp)}, device_id_type=MESH
        )
    pl.semaphore_wait(barrier, ndp - 1)

    def rows(j):
        return pl.ds(pl.multiple_of(j * tok, tok), tok)

    def span(c):
        return pl.ds(c * piece, piece)

    def send(src, owner, c, sem, target):
        pltpu.make_async_remote_copy(
            src_ref=src,
            dst_ref=g_in.at[rows(owner), span(c)],
            send_sem=sem,
            recv_sem=g_recv.at[owner, c],
            device_id={"dp": target},
            device_id_type=MESH,
        ).start()

    for c in range(parts):
        for k in range(1, ny):
            send(g_ref.at[:, span(c)], me, c, far_send.at[k], lax.rem(y + k, ny) * 2 + core)
        send(g_ref.at[:, span(c)], me, c, near_send, partner)

    def arrive(owner, c):
        wait_bytes(g_in.at[rows(owner), span(c)], g_recv.at[owner, c])

    mine = pl.ds(pl.multiple_of(me * share, share), share)

    def multiply(src, owner):
        def tile(i, carry):
            cols = pl.ds(pl.multiple_of(i * 256, 256), 256)
            outs[rows(owner), cols] = jnp.dot(
                src[...], w_ref[:, cols], preferred_element_type=jnp.float32
            ).astype(jnp.bfloat16)
            return carry

        lax.fori_loop(0, share // 256, tile, 0)

    def answer(owner):
        multiply(g_in.at[rows(owner), :], owner)
        pltpu.make_async_remote_copy(
            src_ref=outs.at[rows(owner), :],
            dst_ref=proj.at[:, mine],
            send_sem=r_send.at[owner],
            recv_sem=r_recv.at[me],
            device_id={"dp": owner},
            device_id_type=MESH,
        ).start()

    multiply(g_ref, me)
    proj[:, mine] = outs[rows(me), :]

    for c in range(parts):
        arrive(partner, c)
    answer(partner)

    def source(k):
        return lax.rem(y + ny - k, ny) * 2

    for c in range(parts):
        for k in range(1, ny):
            owner = source(k) + core
            arrive(owner, c)
            send(g_in.at[rows(owner), span(c)], owner, c, relay_send.at[k], partner)
    for k in range(1, ny):
        answer(source(k) + core)
    for k in range(1, ny):
        owner = source(k) + 1 - core
        for c in range(parts):
            arrive(owner, c)
        answer(owner)
    for k in range(1, ndp):
        owner = lax.rem(me + k, ndp)
        cols = pl.ds(pl.multiple_of(owner * share, share), share)
        wait_bytes(proj.at[:, cols], r_recv.at[owner])
    hidden = (res_ref[...].astype(jnp.float32) + proj[...].astype(jnp.float32)).astype(jnp.bfloat16)
    hid_ref[...] = hidden
    hidden_f = hidden.astype(jnp.float32)
    scale = lax.rsqrt(jnp.mean(hidden_f * hidden_f, axis=-1, keepdims=True) + NORM_EPS)
    moe_ref[...] = (hidden_f * scale * gain_ref[...]).astype(jnp.bfloat16)
    for k in range(1, ny):
        wait_bytes(g_ref, far_send.at[k])
        wait_bytes(g_ref, relay_send.at[k])
    wait_bytes(g_ref, near_send)
    for k in range(1, ndp):
        owner = lax.rem(me + k, ndp)
        wait_bytes(outs.at[rows(owner), :], r_send.at[owner])


def project(gated, weight, residual, gain):
    ndp = lax.axis_size("dp")
    tok, wide = gated.shape
    share = weight.shape[1]
    model = residual.shape[1]
    bf16 = jnp.bfloat16
    dma = pltpu.SemaphoreType.DMA
    return pl.pallas_call(
        functools.partial(project_kernel, ndp, GATED_PARTS),
        out_shape=[jax.ShapeDtypeStruct((tok, model), bf16)] * 2,
        in_specs=[VMEM_WHOLE] * 4,
        out_specs=[VMEM_WHOLE] * 2,
        scratch_shapes=[
            pltpu.VMEM((ndp * tok, wide), bf16),
            pltpu.VMEM((ndp * tok, share), bf16),
            pltpu.VMEM((tok, model), bf16),
            dma((ndp,)),
            dma,
            dma((ndp,)),
            dma((ndp, GATED_PARTS)),
            dma((ndp,)),
            dma((ndp,)),
        ],
        compiler_params=pltpu.CompilerParams(
            collective_id=4, has_side_effects=True, vmem_limit_bytes=32 * 1024 * 1024
        ),
    )(gated, weight, residual, gain)


def local(
    queries,
    forget_pre,
    values,
    out_gate,
    lower_bound,
    head_gain,
    residual,
    out_weight,
    ffn_gain,
    routing,
    route_weight,
    expert_gate,
    expert_up,
    expert_down,
):
    tok_rows = queries.shape[1]
    model_width = residual.shape[2]
    top_count = routing.shape[2]
    span_sp = lax.axis_size("sp")
    span_dp = lax.axis_size("dp")
    experts = expert_gate.shape[0] * span_sp * span_dp
    cap = max(2, 5 * tok_rows * top_count // (4 * experts))
    nx = span_dp // 2
    nz = span_sp // nx
    per = -(-nz * cap // 16) * 16
    width = min(CHUNK, model_width)
    pack = jnp.concatenate([routing[0].astype(jnp.float32), route_weight[0]], axis=1).T
    gated, packed = mixer(
        queries[0],
        forget_pre[0],
        values[0],
        out_gate[0],
        lower_bound[None, :],
        pack,
        head_gain[None, :],
    )
    hidden, moe_in = project(gated, out_weight, residual[0], ffn_gain[None, :])
    act = dispatch(
        moe_in, packed, expert_gate[0], expert_up[0], nz, nx, span_dp, width, cap, per
    )
    layer_out = combine(act, expert_down[0], packed, hidden, nz, nx, span_dp, width, cap)
    return layer_out.reshape(1, tok_rows, model_width)


def solution(mesh):
    in_specs = (
        P("dp", "sp", None),
        P("dp", "sp", None),
        P("dp", "sp", None),
        P("dp", "sp", None),
        P("sp"),
        P(),
        P("dp", "sp", None),
        P(None, "dp"),
        P(),
        P("dp", "sp", None),
        P("dp", "sp", None),
        P(("sp", "dp"), None, None),
        P(("sp", "dp"), None, None),
        P(("sp", "dp"), None, None),
    )
    out_specs = P("dp", "sp", None)
    return jax.shard_map(local, mesh=mesh, in_specs=in_specs, out_specs=out_specs, check_vma=False)
```

```python
import functools

import jax
import jax.numpy as jnp
from jax import lax
from jax.experimental import pallas as pl
from jax.experimental.pallas import tpu as pltpu
from jax.sharding import PartitionSpec as P

MESH = pl.DeviceIdType.MESH
VMEM_WHOLE = pl.BlockSpec(memory_space=pltpu.VMEM)

CHUNK = 256
GATED_PARTS = 4


NORM_EPS = 1e-06


def wait_bytes(ref, sem):
    pltpu.make_async_copy(ref, ref, sem).wait()


def place(nz, nx, ndp):
    sp, dp = lax.axis_index("sp"), lax.axis_index("dp")
    z = lax.div(sp, nx)
    me = lax.rem(sp, nx) * ndp + dp
    above, below = {"sp": sp + nx, "dp": dp}, {"sp": sp - nx, "dp": dp}

    def member(p):
        return {"sp": z * nx + lax.div(p, ndp), "dp": lax.rem(p, ndp)}

    return z, me, above, below, member


def greet(nz, peers, z, me, above, below, member):
    barrier = pltpu.get_barrier_semaphore()

    @pl.when(z > 0)
    def _():
        pl.semaphore_signal(barrier, inc=1, device_id=below, device_id_type=MESH)

    @pl.when(z < nz - 1)
    def _():
        pl.semaphore_signal(barrier, inc=1, device_id=above, device_id_type=MESH)

    def one(k, carry):
        pl.semaphore_signal(
            barrier, inc=1, device_id=member(lax.rem(me + k, peers)), device_id_type=MESH
        )
        return carry

    lax.fori_loop(1, peers, one, 0)
    count = peers - 1 + jnp.where(z > 0, 1, 0) + jnp.where(z < nz - 1, 1, 0)
    pl.semaphore_wait(barrier, count)


def routing_tables(packed_ref, nz, nx, ndp, cap):
    peers = nx * ndp
    _, double, tok = packed_ref.shape
    top = double // 2
    sp = lax.axis_index("sp")
    z, x = lax.div(sp, nx), lax.rem(sp, nx)
    ids = lax.broadcasted_iota(jnp.int32, (peers, tok), 0) + z * peers
    row = lax.broadcasted_iota(jnp.int32, (tok, tok), 0)
    col = lax.broadcasted_iota(jnp.int32, (tok, tok), 1)
    earlier = jnp.where(row < col, 1.0, 0.0).astype(jnp.bfloat16)
    found = []
    for b in range(nz):
        item = packed_ref[b * nx + x]
        chosen = item[:top].astype(jnp.int32)
        named = jnp.zeros((peers, tok), jnp.float32)
        weight = jnp.zeros((peers, tok), jnp.float32)
        for j in range(top):
            same = chosen[j : j + 1] == ids
            named = jnp.where(same, 1.0, named)
            weight = jnp.where(same, item[top + j : top + j + 1], weight)
        rank = jnp.dot(named.astype(jnp.bfloat16), earlier, preferred_element_type=jnp.float32)
        slot = jnp.where(named > 0, b * cap + rank.astype(jnp.int32), -1)
        found.append((slot, weight))
    return found


def dispatch_kernel(
    nz,
    nx,
    ndp,
    width,
    cap,
    x_ref,
    packed_ref,
    gate_ref,
    lift_ref,
    act_ref,
    pick_ref,
    gath,
    slots,
    got,
    gate_sum,
    lift_sum,
    up_send,
    dn_send,
    line_recv,
    pl_send,
    pl_recv,
):
    peers = nx * ndp
    z, me, above, below, member = place(nz, nx, ndp)
    tok, model = x_ref.shape
    chunks = model // width
    per = act_ref.shape[0] // peers
    greet(nz, peers, z, me, above, below, member)

    def block(b):
        return pl.ds(pl.multiple_of(b * tok, tok), tok)

    def share(p):
        return pl.ds(pl.multiple_of(p * per, per), per)

    def pass_on(src, b, c, cols, sem, device):
        pltpu.make_async_remote_copy(
            src_ref=src,
            dst_ref=gath.at[block(b), cols],
            send_sem=sem,
            recv_sem=line_recv.at[b, c],
            device_id=device,
            device_id_type=MESH,
        ).start()

    gath[block(z), :] = x_ref[...]
    slot_ids = lax.broadcasted_iota(jnp.int32, (per, tok), 0)
    for b, (slot, _) in enumerate(routing_tables(packed_ref, nz, nx, ndp, cap)):
        for p in range(peers):
            pick_ref[p * per : (p + 1) * per, b * tok : (b + 1) * tok] = jnp.where(
                slot_ids == slot[p : p + 1], 1.0, 0.0
            ).astype(jnp.bfloat16)
    gate_sum[...] = jnp.zeros_like(gate_sum)
    lift_sum[...] = jnp.zeros_like(lift_sum)

    def tick(t, carry):
        for s in range(nz):
            c = t - s
            cols = pl.ds(pl.multiple_of(c * width, width), width)
            valid = (c >= 0) & (c < chunks)
            if s == 0:

                @pl.when(valid & (z < nz - 1))
                def _():
                    pass_on(x_ref.at[:, cols], z, c, cols, up_send.at[0], above)

                @pl.when(valid & (z > 0))
                def _():
                    pass_on(x_ref.at[:, cols], z, c, cols, dn_send.at[0], below)

                continue

            @pl.when(valid & (z - s >= 0))
            def _():
                b = z - s
                here = gath.at[block(b), cols]
                wait_bytes(here, line_recv.at[b, c])

                @pl.when(z < nz - 1)
                def _():
                    pass_on(here, b, c, cols, up_send.at[s], above)

            @pl.when(valid & (z + s < nz))
            def _():
                b = z + s
                here = gath.at[block(b), cols]
                wait_bytes(here, line_recv.at[b, c])

                @pl.when(z > 0)
                def _():
                    pass_on(here, b, c, cols, dn_send.at[s], below)

        c = t - (nz - 1)

        @pl.when((c >= 0) & (c < chunks))
        def _():
            cols = pl.ds(pl.multiple_of(c * width, width), width)
            slots[:, cols] = jnp.dot(
                pick_ref[...], gath[:, cols], preferred_element_type=jnp.float32
            ).astype(jnp.bfloat16)
            got[share(me), cols] = slots[share(me), cols]

            def send(k, inner):
                p = lax.rem(me + k, peers)
                pltpu.make_async_remote_copy(
                    src_ref=slots.at[share(p), cols],
                    dst_ref=got.at[share(me), cols],
                    send_sem=pl_send.at[k],
                    recv_sem=pl_recv.at[k, c],
                    device_id=member(p),
                    device_id_type=MESH,
                ).start()
                return inner

            lax.fori_loop(1, peers, send, 0)

        late = t - nz

        @pl.when(late >= 0)
        def _():
            cols = pl.ds(pl.multiple_of(late * width, width), width)

            def arrive(k, inner):
                p = lax.rem(me + peers - k, peers)
                wait_bytes(got.at[share(p), cols], pl_recv.at[k, late])
                return inner

            lax.fori_loop(1, peers, arrive, 0)
            rows = got[:, cols]
            gate_sum[...] += jnp.dot(rows, gate_ref[cols, :], preferred_element_type=jnp.float32)
            lift_sum[...] += jnp.dot(rows, lift_ref[cols, :], preferred_element_type=jnp.float32)

        return carry

    lax.fori_loop(0, chunks + nz, tick, 0)
    gate = gate_sum[...]
    act_ref[...] = (gate / (1.0 + jnp.exp(-gate)) * lift_sum[...]).astype(jnp.bfloat16)

    for s in range(nz - 1):

        @pl.when((z - s >= 0) & (z < nz - 1))
        def _():
            wait_bytes(x_ref, up_send.at[s])

        @pl.when((z + s < nz) & (z > 0))
        def _():
            wait_bytes(x_ref, dn_send.at[s])

    def finish(k, carry):
        wait_bytes(slots.at[share(lax.rem(me + k, peers)), :], pl_send.at[k])
        return carry

    lax.fori_loop(1, peers, finish, 0)


def return_kernel(
    nz,
    nx,
    ndp,
    width,
    cap,
    act_ref,
    down_ref,
    packed_ref,
    h_ref,
    out_ref,
    mixed,
    high_ref,
    low_ref,
    r_ref,
    ret,
    part,
    up_out,
    up_in,
    dn_out,
    dn_in,
    pl_send,
    pl_recv,
    up_send,
    dn_send,
    up_recv,
    dn_recv,
):
    peers = nx * ndp
    z, me, above, below, member = place(nz, nx, ndp)
    tok, model = h_ref.shape
    chunks = model // width
    per = r_ref.shape[0] // peers
    greet(nz, peers, z, me, above, below, member)

    def block(b):
        return pl.ds(pl.multiple_of(b * tok, tok), tok)

    def share(p):
        return pl.ds(pl.multiple_of(p * per, per), per)

    def columns(c):
        return pl.ds(pl.multiple_of(c * width, width), width)

    def send_chunk(c, carry):
        r_ref[:, columns(c)] = jnp.dot(
            act_ref[...], down_ref[:, columns(c)], preferred_element_type=jnp.float32
        ).astype(jnp.bfloat16)

        def send(k, inner):
            p = lax.rem(me + k, peers)
            pltpu.make_async_remote_copy(
                src_ref=r_ref.at[share(p), columns(c)],
                dst_ref=ret.at[share(me), columns(c)],
                send_sem=pl_send.at[k],
                recv_sem=pl_recv.at[k, c],
                device_id=member(p),
                device_id_type=MESH,
            ).start()
            return inner

        return lax.fori_loop(1, peers, send, carry)

    lax.fori_loop(0, chunks, send_chunk, 0)
    ret[share(me), :] = r_ref[share(me), :]
    slot_ids = lax.broadcasted_iota(jnp.int32, (per, tok), 0)
    for b, (slot, weight) in enumerate(routing_tables(packed_ref, nz, nx, ndp, cap)):
        for p in range(peers):
            mixed[p * per : (p + 1) * per, b * tok : (b + 1) * tok] = jnp.where(
                slot_ids == slot[p : p + 1], weight[p : p + 1], 0.0
            )
    turned = mixed[...].T
    high = turned.astype(jnp.bfloat16)
    high_ref[...] = high
    low_ref[...] = (turned - high.astype(jnp.float32)).astype(jnp.bfloat16)

    def line(order, c, first, sends, takes, inbox, outbox, send_sem, recv_sem, device):
        cols = columns(c)
        for d in order:
            rows = pl.ds(d * tok, tok)

            @pl.when(jnp.logical_not(first) & takes(d))
            def _():
                wait_bytes(inbox.at[rows, cols], recv_sem.at[d, c])

            @pl.when(sends(d))
            def _():
                @pl.when(first)
                def _():
                    outbox[rows, cols] = part[rows, cols].astype(jnp.bfloat16)

                @pl.when(jnp.logical_not(first))
                def _():
                    outbox[rows, cols] = (
                        part[rows, cols] + inbox[rows, cols].astype(jnp.float32)
                    ).astype(jnp.bfloat16)

                pltpu.make_async_remote_copy(
                    src_ref=outbox.at[rows, cols],
                    dst_ref=inbox.at[rows, cols],
                    send_sem=send_sem.at[d],
                    recv_sem=recv_sem.at[d, c],
                    device_id=device,
                    device_id_type=MESH,
                ).start()

    def tick(t, carry):
        @pl.when(t < chunks)
        def _():
            cols = columns(t)

            def arrive(k, inner):
                p = lax.rem(me + peers - k, peers)
                wait_bytes(ret.at[share(p), cols], pl_recv.at[k, t])
                return inner

            lax.fori_loop(1, peers, arrive, 0)
            rows = ret[:, cols]
            part[:, cols] = jnp.dot(
                high_ref[...], rows, preferred_element_type=jnp.float32
            ) + jnp.dot(low_ref[...], rows, preferred_element_type=jnp.float32)

        cu = t - z

        @pl.when((cu >= 0) & (cu < chunks))
        def _():
            line(
                range(nz - 1, -1, -1),
                cu,
                z == 0,
                lambda d: d > z,
                lambda d: d >= z,
                up_in,
                up_out,
                up_send,
                up_recv,
                above,
            )

        cd = t - (nz - 1 - z)

        @pl.when((cd >= 0) & (cd < chunks))
        def _():
            line(
                range(nz),
                cd,
                z == nz - 1,
                lambda d: d < z,
                lambda d: d <= z,
                dn_in,
                dn_out,
                dn_send,
                dn_recv,
                below,
            )

        return carry

    lax.fori_loop(0, chunks + nz - 1, tick, 0)

    own = block(z)

    @pl.when(z > 0)
    def _():
        part[own, :] = part[own, :] + up_in[own, :].astype(jnp.float32)

    @pl.when(z < nz - 1)
    def _():
        part[own, :] = part[own, :] + dn_in[own, :].astype(jnp.float32)

    out_ref[...] = (h_ref[...].astype(jnp.float32) + part[own, :]).astype(jnp.bfloat16)

    for d in range(nz):

        @pl.when(d > z)
        def _():
            wait_bytes(up_out.at[pl.ds(d * tok, tok), :], up_send.at[d])

        @pl.when(d < z)
        def _():
            wait_bytes(dn_out.at[pl.ds(d * tok, tok), :], dn_send.at[d])

    def finish(k, carry):
        wait_bytes(r_ref.at[share(lax.rem(me + k, peers)), :], pl_send.at[k])
        return carry

    lax.fori_loop(1, peers, finish, 0)


def dispatch(moe_in, packed, w_gate, w_up, nz, nx, ndp, width, cap, per):
    tok, model = moe_in.shape
    inner = w_gate.shape[1]
    peers = nx * ndp
    total = peers * per
    chunks = model // width
    bf16 = jnp.bfloat16
    return pl.pallas_call(
        functools.partial(dispatch_kernel, nz, nx, ndp, width, cap),
        out_shape=jax.ShapeDtypeStruct((total, inner), bf16),
        in_specs=[VMEM_WHOLE] * 4,
        out_specs=VMEM_WHOLE,
        scratch_shapes=[
            pltpu.VMEM((total, nz * tok), bf16),
            pltpu.VMEM((nz * tok, model), bf16),
            pltpu.VMEM((total, model), bf16),
            pltpu.VMEM((total, model), bf16),
            pltpu.VMEM((total, inner), jnp.float32),
            pltpu.VMEM((total, inner), jnp.float32),
            pltpu.SemaphoreType.DMA((nz,)),
            pltpu.SemaphoreType.DMA((nz,)),
            pltpu.SemaphoreType.DMA((nz, chunks)),
            pltpu.SemaphoreType.DMA((peers,)),
            pltpu.SemaphoreType.DMA((peers, chunks)),
        ],
        compiler_params=pltpu.CompilerParams(
            collective_id=1, has_side_effects=True, vmem_limit_bytes=60 * 1024 * 1024
        ),
        cost_estimate=spent(6 * total * model * inner, total * model * nz),
    )(moe_in, packed, w_gate, w_up)


def combine(act, w_down, packed, hidden, nz, nx, ndp, width, cap):
    tok, model = hidden.shape
    peers = nx * ndp
    total = act.shape[0]
    chunks = model // width
    bf16 = jnp.bfloat16
    return pl.pallas_call(
        functools.partial(return_kernel, nz, nx, ndp, width, cap),
        out_shape=jax.ShapeDtypeStruct((tok, model), bf16),
        in_specs=[VMEM_WHOLE] * 4,
        out_specs=VMEM_WHOLE,
        scratch_shapes=[
            pltpu.VMEM((total, nz * tok), jnp.float32),
            pltpu.VMEM((nz * tok, total), bf16),
            pltpu.VMEM((nz * tok, total), bf16),
            pltpu.VMEM((total, model), bf16),
            pltpu.VMEM((total, model), bf16),
            pltpu.VMEM((nz * tok, model), jnp.float32),
            pltpu.VMEM((nz * tok, model), bf16),
            pltpu.VMEM((nz * tok, model), bf16),
            pltpu.VMEM((nz * tok, model), bf16),
            pltpu.VMEM((nz * tok, model), bf16),
            pltpu.SemaphoreType.DMA((peers,)),
            pltpu.SemaphoreType.DMA((peers, chunks)),
            pltpu.SemaphoreType.DMA((nz,)),
            pltpu.SemaphoreType.DMA((nz,)),
            pltpu.SemaphoreType.DMA((nz, chunks)),
            pltpu.SemaphoreType.DMA((nz, chunks)),
        ],
        compiler_params=pltpu.CompilerParams(
            collective_id=2, has_side_effects=True, vmem_limit_bytes=60 * 1024 * 1024
        ),
        cost_estimate=spent(6 * nz * tok * total * model, total * model * nz),
    )(act, w_down, packed, hidden)


def spent(flops, moved):
    return pl.CostEstimate(flops=4 * flops, bytes_accessed=16 * moved, transcendentals=0)


def mixer_kernel(
    n,
    q_ref,
    f_ref,
    v_ref,
    og_ref,
    own_bound_ref,
    own_pack_ref,
    gain_ref,
    out_ref,
    pack_ref,
    bound_in,
    qs,
    qr,
    ks,
    kr,
    within,
    push,
    keep,
    push_in,
    keep_in,
    before_out,
    before_in,
    bound_send,
    pack_send,
    bound_recv,
    pack_recv,
    push_send,
    keep_send,
    push_recv,
    keep_recv,
    back_send,
    back_recv,
):
    me = lax.axis_index("sp")
    bf16, f32 = jnp.bfloat16, jnp.float32
    tok, _ = q_ref.shape
    heads, size, _ = push.shape
    own = heads // n
    barrier = pltpu.get_barrier_semaphore()

    def other(k):
        return lax.rem(me + k, n)

    def greet_one(k, carry):
        pl.semaphore_signal(barrier, inc=1, device_id={"sp": other(k)}, device_id_type=MESH)
        return carry

    lax.fori_loop(1, n, greet_one, 0)

    bound_in[me] = own_bound_ref[...]
    pack_ref[me] = own_pack_ref[...]
    pl.semaphore_wait(barrier, n - 1)

    def spread(k, carry):
        for src, dst, send_sem, recv_sem in (
            (own_bound_ref, bound_in, bound_send, bound_recv),
            (own_pack_ref, pack_ref, pack_send, pack_recv),
        ):
            pltpu.make_async_remote_copy(
                src_ref=src,
                dst_ref=dst.at[me],
                send_sem=send_sem.at[k],
                recv_sem=recv_sem.at[me],
                device_id={"sp": other(k)},
                device_id_type=MESH,
            ).start()
        return carry

    lax.fori_loop(1, n, spread, 0)

    row = lax.broadcasted_iota(jnp.int32, (tok, tok), 0)
    col = lax.broadcasted_iota(jnp.int32, (tok, tok), 1)
    causal = row >= col
    lower = jnp.where(causal, 1.0, 0.0).astype(bf16)

    def columns(h):
        return pl.ds(pl.multiple_of(h * size, size), size)

    def group(j):
        return pl.ds(j * own, own)

    def halves(value):
        first = value.astype(bf16)
        return first, (value - first.astype(f32)).astype(bf16)

    def prepare(j, carry):
        @pl.when(j != me)
        def _():
            wait_bytes(bound_in.at[j], bound_recv.at[j])

        for i in range(own):
            h = j * own + i
            cols = columns(h)
            bound = bound_in[j][:, i * size : (i + 1) * size]
            forget = f_ref[:, cols].astype(f32)
            leak = (1.0 - bound) / (1.0 + jnp.exp(forget))
            log_keep = jnp.log1p(-leak)
            first = log_keep.astype(bf16)
            second, third = halves(log_keep - first.astype(f32))
            log_run = (
                jnp.dot(lower, first, preferred_element_type=f32)
                + jnp.dot(lower, second, preferred_element_type=f32)
                + jnp.dot(lower, third, preferred_element_type=f32)
            )
            last = log_run[tok - 1 : tok, :]
            ks[:, cols], kr[:, cols] = halves(leak * jnp.exp(-log_run))
            qs[:, cols], qr[:, cols] = halves(q_ref[:, cols].astype(f32) * jnp.exp(log_run))
            total = jnp.zeros((size, size), f32)
            for term in halves(leak * jnp.exp(last - log_run)):
                total = total + lax.dot_general(
                    v_ref[:, cols], term, (((0,), (0,)), ((), ())), preferred_element_type=f32
                )
            push[h] = total.astype(bf16)
            keep[h] = jnp.broadcast_to(jnp.exp(last), (8, size))
        return carry

    lax.fori_loop(0, n, prepare, 0)

    def send_push(k, carry):
        j = other(k)
        pltpu.make_async_remote_copy(
            src_ref=push.at[group(j)],
            dst_ref=push_in.at[group(me)],
            send_sem=push_send.at[k],
            recv_sem=push_recv.at[me],
            device_id={"sp": j},
            device_id_type=MESH,
        ).start()
        pltpu.make_async_remote_copy(
            src_ref=keep.at[group(j)],
            dst_ref=keep_in.at[group(me)],
            send_sem=keep_send.at[k],
            recv_sem=keep_recv.at[me],
            device_id={"sp": j},
            device_id_type=MESH,
        ).start()
        return carry

    lax.fori_loop(1, n, send_push, 0)
    push_in[group(me)] = push[group(me)]
    keep_in[group(me)] = keep[group(me)]

    def across(a, b):
        return lax.dot_general(a, b, (((1,), (1,)), ((), ())), preferred_element_type=f32)

    def inside(j, carry):
        for i in range(own):
            cols = columns(j * own + i)
            scores = (
                across(qs[:, cols], ks[:, cols])
                + across(qs[:, cols], kr[:, cols])
                + across(qr[:, cols], ks[:, cols])
            )
            first, second = halves(jnp.where(causal, scores, 0.0))
            within[:, cols] = jnp.dot(
                first, v_ref[:, cols], preferred_element_type=f32
            ) + jnp.dot(second, v_ref[:, cols], preferred_element_type=f32)
        return carry

    lax.fori_loop(0, n, inside, 0)

    def scan(b, states):
        @pl.when(b != me)
        def _():
            wait_bytes(push_in.at[group(b)], push_recv.at[b])
            wait_bytes(keep_in.at[group(b)], keep_recv.at[b])

        for i in range(own):
            before_out[b * own + i] = states[i].astype(bf16)

        @pl.when(b != me)
        def _():
            pltpu.make_async_remote_copy(
                src_ref=before_out.at[group(b)],
                dst_ref=before_in.at[group(me)],
                send_sem=back_send.at[b],
                recv_sem=back_recv.at[me],
                device_id={"sp": b},
                device_id_type=MESH,
            ).start()

        @pl.when(b == me)
        def _():
            before_in[group(me)] = before_out[group(me)]

        return tuple(
            states[i] * keep_in[b * own + i][0:1, :] + push_in[b * own + i].astype(f32)
            for i in range(own)
        )

    lax.fori_loop(0, n, scan, tuple(jnp.zeros((size, size), f32) for _ in range(own)))

    def settle(k, carry):
        j = other(k)
        wait_bytes(before_in.at[group(j)], back_recv.at[j])
        return carry

    lax.fori_loop(1, n, settle, 0)

    def close(j, carry):
        for i in range(own):
            h = j * own + i
            cols = columns(h)
            mix = (
                within[:, cols]
                + across(qs[:, cols], before_in[h])
                + across(qr[:, cols], before_in[h])
            )
            scale = lax.rsqrt(jnp.mean(mix * mix, axis=-1, keepdims=True) + NORM_EPS)
            normed = (mix * scale * gain_ref[...]).astype(bf16).astype(f32)
            gate = og_ref[:, cols].astype(f32)
            out_ref[:, cols] = (normed * (gate / (1.0 + jnp.exp(-gate)))).astype(bf16)
        return carry

    lax.fori_loop(0, n, close, 0)

    def finish(k, carry):
        j = other(k)
        wait_bytes(pack_ref.at[j], pack_recv.at[j])
        wait_bytes(own_pack_ref, pack_send.at[k])
        wait_bytes(own_bound_ref, bound_send.at[k])
        wait_bytes(push.at[group(j)], push_send.at[k])
        wait_bytes(keep.at[group(j)], keep_send.at[k])
        wait_bytes(before_out.at[group(j)], back_send.at[j])
        return carry

    lax.fori_loop(1, n, finish, 0)


def mixer(q, f, v, og, bound, pack, gain):
    n = lax.axis_size("sp")
    tok, wide = q.shape
    size = gain.shape[1]
    heads = wide // size
    bf16 = jnp.bfloat16
    states = pltpu.VMEM((heads, size, size), bf16)
    keeps = pltpu.VMEM((heads, 8, size), jnp.float32)
    return pl.pallas_call(
        functools.partial(mixer_kernel, n),
        out_shape=[
            jax.ShapeDtypeStruct((tok, wide), bf16),
            jax.ShapeDtypeStruct((n,) + pack.shape, jnp.float32),
        ],
        in_specs=[VMEM_WHOLE] * 7,
        out_specs=[VMEM_WHOLE] * 2,
        scratch_shapes=[
            pltpu.VMEM((n,) + bound.shape, jnp.float32),
            pltpu.VMEM((tok, wide), bf16),
            pltpu.VMEM((tok, wide), bf16),
            pltpu.VMEM((tok, wide), bf16),
            pltpu.VMEM((tok, wide), bf16),
            pltpu.VMEM((tok, wide), jnp.float32),
            states,
            keeps,
            states,
            keeps,
            states,
            states,
        ]
        + [pltpu.SemaphoreType.DMA((n,))] * 10,
        compiler_params=pltpu.CompilerParams(
            collective_id=3, has_side_effects=True, vmem_limit_bytes=32 * 1024 * 1024
        ),
        cost_estimate=spent(24 * tok * wide * size, 8 * tok * wide),
    )(q, f, v, og, bound, pack, gain)


def project_kernel(
    ndp,
    parts,
    g_ref,
    w_ref,
    res_ref,
    gain_ref,
    hid_ref,
    moe_ref,
    g_in,
    outs,
    proj,
    far_send,
    near_send,
    relay_send,
    g_recv,
    r_send,
    r_recv,
):
    me = lax.axis_index("dp")
    tok, wide = g_ref.shape
    share = w_ref.shape[1]
    ny = ndp // 2
    y, core = lax.div(me, 2), lax.rem(me, 2)
    partner = y * 2 + 1 - core
    piece = wide // parts
    barrier = pltpu.get_barrier_semaphore()
    for k in range(1, ndp):
        pl.semaphore_signal(
            barrier, inc=1, device_id={"dp": lax.rem(me + k, ndp)}, device_id_type=MESH
        )
    pl.semaphore_wait(barrier, ndp - 1)

    def rows(j):
        return pl.ds(pl.multiple_of(j * tok, tok), tok)

    def span(c):
        return pl.ds(c * piece, piece)

    def send(src, owner, c, sem, target):
        pltpu.make_async_remote_copy(
            src_ref=src,
            dst_ref=g_in.at[rows(owner), span(c)],
            send_sem=sem,
            recv_sem=g_recv.at[owner, c],
            device_id={"dp": target},
            device_id_type=MESH,
        ).start()

    for c in range(parts):
        for k in range(1, ny):
            send(g_ref.at[:, span(c)], me, c, far_send.at[k], lax.rem(y + k, ny) * 2 + core)
        send(g_ref.at[:, span(c)], me, c, near_send, partner)

    def arrive(owner, c):
        wait_bytes(g_in.at[rows(owner), span(c)], g_recv.at[owner, c])

    mine = pl.ds(pl.multiple_of(me * share, share), share)

    def multiply(src, owner):
        def tile(i, carry):
            cols = pl.ds(pl.multiple_of(i * 256, 256), 256)
            outs[rows(owner), cols] = jnp.dot(
                src[...], w_ref[:, cols], preferred_element_type=jnp.float32
            ).astype(jnp.bfloat16)
            return carry

        lax.fori_loop(0, share // 256, tile, 0)

    def answer(owner):
        multiply(g_in.at[rows(owner), :], owner)
        pltpu.make_async_remote_copy(
            src_ref=outs.at[rows(owner), :],
            dst_ref=proj.at[:, mine],
            send_sem=r_send.at[owner],
            recv_sem=r_recv.at[me],
            device_id={"dp": owner},
            device_id_type=MESH,
        ).start()

    multiply(g_ref, me)
    proj[:, mine] = outs[rows(me), :]

    for c in range(parts):
        arrive(partner, c)
    answer(partner)

    def source(k):
        return lax.rem(y + ny - k, ny) * 2

    for c in range(parts):
        for k in range(1, ny):
            owner = source(k) + core
            arrive(owner, c)
            send(g_in.at[rows(owner), span(c)], owner, c, relay_send.at[k], partner)
    for k in range(1, ny):
        answer(source(k) + core)
    for k in range(1, ny):
        owner = source(k) + 1 - core
        for c in range(parts):
            arrive(owner, c)
        answer(owner)
    for k in range(1, ndp):
        owner = lax.rem(me + k, ndp)
        cols = pl.ds(pl.multiple_of(owner * share, share), share)
        wait_bytes(proj.at[:, cols], r_recv.at[owner])
    hidden = (res_ref[...].astype(jnp.float32) + proj[...].astype(jnp.float32)).astype(jnp.bfloat16)
    hid_ref[...] = hidden
    hidden_f = hidden.astype(jnp.float32)
    scale = lax.rsqrt(jnp.mean(hidden_f * hidden_f, axis=-1, keepdims=True) + NORM_EPS)
    moe_ref[...] = (hidden_f * scale * gain_ref[...]).astype(jnp.bfloat16)
    for k in range(1, ny):
        wait_bytes(g_ref, far_send.at[k])
        wait_bytes(g_ref, relay_send.at[k])
    wait_bytes(g_ref, near_send)
    for k in range(1, ndp):
        owner = lax.rem(me + k, ndp)
        wait_bytes(outs.at[rows(owner), :], r_send.at[owner])


def project(gated, weight, residual, gain):
    ndp = lax.axis_size("dp")
    tok, wide = gated.shape
    share = weight.shape[1]
    model = residual.shape[1]
    bf16 = jnp.bfloat16
    dma = pltpu.SemaphoreType.DMA
    return pl.pallas_call(
        functools.partial(project_kernel, ndp, GATED_PARTS),
        out_shape=[jax.ShapeDtypeStruct((tok, model), bf16)] * 2,
        in_specs=[VMEM_WHOLE] * 4,
        out_specs=[VMEM_WHOLE] * 2,
        scratch_shapes=[
            pltpu.VMEM((ndp * tok, wide), bf16),
            pltpu.VMEM((ndp * tok, share), bf16),
            pltpu.VMEM((tok, model), bf16),
            dma((ndp,)),
            dma,
            dma((ndp,)),
            dma((ndp, GATED_PARTS)),
            dma((ndp,)),
            dma((ndp,)),
        ],
        compiler_params=pltpu.CompilerParams(
            collective_id=4, has_side_effects=True, vmem_limit_bytes=32 * 1024 * 1024
        ),
        cost_estimate=spent(2 * ndp * tok * wide * share, 2 * wide * share),
    )(gated, weight, residual, gain)


def local(
    queries,
    forget_pre,
    values,
    out_gate,
    lower_bound,
    head_gain,
    residual,
    out_weight,
    ffn_gain,
    routing,
    route_weight,
    expert_gate,
    expert_up,
    expert_down,
):
    tok_rows = queries.shape[1]
    model_width = residual.shape[2]
    top_count = routing.shape[2]
    span_sp = lax.axis_size("sp")
    span_dp = lax.axis_size("dp")
    experts = expert_gate.shape[0] * span_sp * span_dp
    cap = max(2, 5 * tok_rows * top_count // (4 * experts))
    nx = span_dp // 2
    nz = span_sp // nx
    per = -(-nz * cap // 16) * 16
    width = min(CHUNK, model_width)
    pack = jnp.concatenate([routing[0].astype(jnp.float32), route_weight[0]], axis=1).T
    gated, packed = mixer(
        queries[0],
        forget_pre[0],
        values[0],
        out_gate[0],
        lower_bound[None, :],
        pack,
        head_gain[None, :],
    )
    hidden, moe_in = project(gated, out_weight, residual[0], ffn_gain[None, :])
    act = dispatch(
        moe_in, packed, expert_gate[0], expert_up[0], nz, nx, span_dp, width, cap, per
    )
    layer_out = combine(act, expert_down[0], packed, hidden, nz, nx, span_dp, width, cap)
    return layer_out.reshape(1, tok_rows, model_width)


def solution(mesh):
    in_specs = (
        P("dp", "sp", None),
        P("dp", "sp", None),
        P("dp", "sp", None),
        P("dp", "sp", None),
        P("sp"),
        P(),
        P("dp", "sp", None),
        P(None, "dp"),
        P(),
        P("dp", "sp", None),
        P("dp", "sp", None),
        P(("sp", "dp"), None, None),
        P(("sp", "dp"), None, None),
        P(("sp", "dp"), None, None),
    )
    out_specs = P("dp", "sp", None)
    return jax.shard_map(local, mesh=mesh, in_specs=in_specs, out_specs=out_specs, check_vma=False)
```
